32 devices in a mesh: sp: 8 (over z, x), tp: 4 (over y, core).
Axes of the slice: x: 2, y: 2, z: 4, core: 2. Of those that a mesh axis runs over, the one named last changes fastest.
Arguments:
- mixer_input: bfloat16 [2048, 1024], P('sp', 'tp'), may hold values from -8 to 8
- decay_shift: float32 [2048, 64], P('sp', 'tp'), may hold values from -2.3 to 0
- pole_real: float32 [64, 64], P('tp'), may hold values from -1 to 0
- pole_imaginary: float32 [64, 64], P('tp'), may hold values from 1 to 201.06176
- log_step: float32 [64], P('tp'), may hold values from -4.15 to -3
- input_map: float32 [2, 64, 64, 16], P(None, 'tp'), may hold values from -1 to 1
- readout_matrix: float32 [2, 64, 16, 64], P(None, 'tp'), may hold values from -0.5 to 0.5
- skip: float32 [1024], P('tp'), may hold values from -6 to 6
- out_proj: bfloat16 [1024, 2048], P('tp'), may hold values from -0.1875 to 0.1875
- stream: bfloat16 [2048, 2048], P(('sp', 'tp')), may hold values from -6 to 6
- norm_gain: float32 [2048], replicated, may hold values from 0.1 to 1.9
- routes: int32 [2048, 2], P(('sp', 'tp')), may hold values from 0 to 7, all different within a row; in each aligned block of 64 rows (0 to 63, 64 to 127, ...) at most 32 rows name the same one
- route_logits: float32 [2048, 2], P(('sp', 'tp')), may hold values from -7.5 to 7.5
- w_gate: bfloat16 [8, 2048, 7168], P('sp', None, 'tp'), may hold values from -0.125 to 0.125
- w_up: bfloat16 [8, 2048, 7168], P('sp', None, 'tp'), may hold values from -0.125 to 0.125
- w_down: bfloat16 [8, 7168, 2048], P('sp', 'tp'), may hold values from -0.21875 to 0.21875
Outputs:
- layer_out: bfloat16 [2048, 2048], P(('sp', 'tp'))
The draws below stay inside these ranges and needn't reach their ends.
Inputs may be any that keep to these rules, and one draw needn't show every extreme that they name: `routes`: in the rows of one device no expert is named more than 32 times, a bound that some block reaches; the 2 experts of a token differ.
All inputs are finite; a program needn't handle non-finite values.
Results may differ from the reference program's by a relative error of at most 0.015.
Values may be sent and summed in bfloat16 or wider, within the bound.
A program may use at most 128 MiB of HBM per device.

```python
import math
import jax
import jax.numpy as jnp
import numpy as np
from jax import lax

D = 2048
GROUPS = 64
GROUP_CH = 16
STATE = 64
EXPERT_FF = 7168
TOP = 2
SEQUENCE_LOCAL = 256
MIXER_CHANNELS = 1024
SEQ = 2048
TOK_DEV = 64
EXPERTS = 8
CAP = 32
N_TP = 4


def quick_groups(key, count):
    order = jax.random.permutation(jax.random.fold_in(key, 101), GROUPS)
    return order < count


def step_logs(key, quick):
    keys = jax.random.split(jax.random.fold_in(key, 211), 2)
    fast = jax.random.uniform(keys[0], (GROUPS,), jnp.float32, -4.15, -3.88)
    slow = jax.random.uniform(keys[1], (GROUPS,), jnp.float32, -3.9, -3.0)
    return jnp.where(quick, fast, slow)


def draw_log_step(key, part):
    count = GROUPS // 2
    return step_logs(key, quick_groups(key, count))


def draw_pole_real(key, part):
    count = GROUPS // 2
    quick = quick_groups(key, count)
    keys = jax.random.split(jax.random.fold_in(key, 11), 2)
    quick_rate = jax.random.uniform(keys[0], (GROUPS, STATE), jnp.float32, 0.6, 1.0)
    slow_rate = jnp.exp(jax.random.uniform(keys[1], (GROUPS, STATE), jnp.float32, math.log(2.0 / SEQ), math.log(20.0 / SEQ)))
    return -jnp.where(quick[:, None], quick_rate, slow_rate)


def draw_pole_imaginary(key, part):
    count = GROUPS // 2
    quick = quick_groups(key, count)
    step = jnp.exp(step_logs(key, quick))
    keys = jax.random.split(jax.random.fold_in(key, 307), 3)
    spread_poles = jax.random.uniform(keys[0], (GROUPS, STATE), jnp.float32, 1.0, 3.14159 * STATE)
    jitter = jax.random.uniform(keys[1], (GROUPS, STATE), jnp.float32, -0.03, 0.03)
    adjusted = jnp.minimum((3.14159 + jitter) / step[:, None], 3.14159 * STATE)
    chosen = jax.random.randint(keys[2], (GROUPS, STATE), 0, 3) == 0
    return jnp.where(quick[:, None] & chosen, adjusted, spread_poles)


def draw_decay_shift(key, part):
    count = GROUPS // 2
    quick = quick_groups(key, count)
    keys = jax.random.split(jax.random.fold_in(key, 23), 5)
    blocks = SEQ // SEQUENCE_LOCAL
    level = jnp.exp(jax.random.uniform(keys[0], (blocks, GROUPS), jnp.float32, math.log(0.25), math.log(2.0)))
    pieces = jnp.exp(jax.random.uniform(keys[1], (SEQ // 32, GROUPS), jnp.float32, math.log(0.5), math.log(2.0)))
    rough = jax.random.uniform(keys[2], (SEQ, GROUPS), jnp.float32, 0.5, 1.5)
    rate = jnp.where(quick, 0.015, 0.8 / SEQ)
    steady = -jnp.repeat(level, SEQUENCE_LOCAL, axis=0) * jnp.repeat(pieces, 32, axis=0) * rough * rate[None, :]
    spots = jax.random.randint(keys[3], (3,), 0, SEQ)
    losses = jax.random.uniform(keys[4], (3, GROUPS), jnp.float32, math.log(0.5), math.log(0.8))
    hits = (jnp.arange(SEQ, dtype=jnp.int32)[:, None] == spots[None, :]).astype(jnp.float32)
    return steady + jnp.dot(hits, losses, precision=lax.Precision.HIGHEST)


def draw_mixer_input(key, part):
    keys = jax.random.split(jax.random.fold_in(key, 401), 2)
    noise = jnp.clip(jax.random.normal(keys[0], (SEQ, MIXER_CHANNELS), jnp.float32), -6.0, 6.0)
    amplitude = jax.random.uniform(keys[1], (MIXER_CHANNELS,), jnp.float32, -2.0, 2.0)
    parity = (1 - 2 * (jnp.arange(SEQ, dtype=jnp.int32) % 2)).astype(jnp.float32)
    return (noise + parity[:, None] * amplitude[None, :]).astype(jnp.bfloat16)


def draw_route_logits(key, part):
    keys = jax.random.split(jax.random.fold_in(key, 503), 3)
    leading = jnp.clip(1.5 * jax.random.normal(keys[0], (SEQ,), jnp.float32), -4.5, 4.5)
    spacing = jax.random.uniform(keys[1], (SEQ,), jnp.float32, 2.0, 3.0)
    direction = (2 * jax.random.randint(keys[2], (SEQ,), 0, 2) - 1).astype(jnp.float32)
    return jnp.stack([leading, leading - direction * spacing], axis=1)


def levels(key, dims, cuts, least, top_value):
    factor_of, own = 1.0, jax.random.fold_in(key, 6)
    for axis_at, parts in cuts:
        heights = jnp.exp(jax.random.uniform(jax.random.fold_in(own, axis_at), (parts,), jnp.float32, least / len(cuts), top_value / len(cuts)))
        factor_of = factor_of * jnp.repeat(heights, dims[axis_at] // parts).reshape([-1 if axis == axis_at else 1 for axis in range(len(dims))])
    return factor_of


def assign_block(rng, own, number, rows, amount, top, most, lean):
    sequence = jax.random.permutation(rng, amount)
    crowded, common = shares(amount, rows * top, most, lean, True), shares(amount, rows * top, most, lean, False)
    places = jnp.arange(amount)

    def named(sizes, offset_by):
        used = int((sizes > 0).sum())
        fixed = max(1, used // 4)
        moved = fixed + (places - fixed + offset_by * (used - fixed)) % max(1, amount - fixed)
        return jnp.zeros((amount,), jnp.int32).at[sequence[jnp.where(places < fixed, places, moved)]].set(jnp.asarray(sizes, jnp.int32))

    sizes = jnp.where(number % 4 == 0, named(crowded, number // 4), named(common, number - number // 4 - 1))
    mixed = jax.random.permutation(jax.random.fold_in(own, 3), amount)
    source_of, receiver = mixed[0:amount // 2 * 2:2], mixed[1:amount // 2 * 2:2]
    slack = jnp.minimum(sizes[source_of] - 1, most - sizes[receiver]) // 2
    slack = jnp.where((source_of == sequence[0]) | (receiver == sequence[0]) | (sizes[receiver] == 0), 0, jnp.maximum(slack, 0))
    moved = jax.random.randint(jax.random.fold_in(own, 4), (amount // 2,), 0, 1 << 20) % (slack + 1)
    sizes = sizes.at[source_of].add(-moved).at[receiver].add(moved)
    items = jnp.searchsorted(jnp.cumsum(sizes), jnp.arange(rows * top), side="right").astype(jnp.int32)
    table = items.reshape(top, rows).T
    table = table[jax.random.permutation(jax.random.fold_in(own, 1), rows)]
    offset_by = jax.random.randint(jax.random.fold_in(own, 2), (rows, 1), 0, top)
    return jnp.take_along_axis(table, (jnp.arange(top)[None, :] + offset_by) % top, axis=1)


def shares(number_of, total, reach, slope, full):
    weights = [(1 << 20) // math.isqrt(rank ** slope) + 1 for rank in range(1, number_of + 1)]
    largest = reach if full else min(reach, max(-(-total // number_of), total * weights[0] // sum(weights)))
    least = 1 if total - largest >= number_of - 1 else 0
    counts, rest = [largest] + [least] * (number_of - 1), total - largest - least * (number_of - 1)
    while rest > 0:
        free = [i for i in range(1, number_of) if counts[i] < largest] or [i for i in range(1, number_of) if counts[i] < reach]
        mass, remaining = sum([weights[i] for i in free]), rest
        for i in free:
            addition = min(reach - counts[i], max(1, remaining * weights[i] // mass), rest)
            counts[i] = counts[i] + addition
            rest = rest - addition
    return np.array(counts)


def gaussian(key, extent, spread, most, cuts=(), kind=jnp.bfloat16):
    factor_of = levels(key, extent, cuts, -0.22, 0.18) if cuts else 1.0
    entries = jax.random.normal(key, extent, jnp.float32) * spread * factor_of
    return jnp.minimum(jnp.maximum(entries, -most), most).astype(kind)


def setup_inputs(seed: int = 0) -> dict:
    key_list = jax.random.split(jax.random.key(seed), 17)
    mixer_input = draw_mixer_input(jax.random.fold_in(key_list[16], 71), 0)
    decay_shift = draw_decay_shift(jax.random.fold_in(key_list[16], 71), 0)
    pole_real = draw_pole_real(jax.random.fold_in(key_list[16], 71), 0)
    pole_imaginary = draw_pole_imaginary(jax.random.fold_in(key_list[16], 71), 0)
    log_step = draw_log_step(jax.random.fold_in(key_list[16], 71), 0)
    input_map = gaussian(key_list[5], (2, GROUPS, STATE, GROUP_CH), (2 * GROUP_CH) ** -0.5, 1.0, ((1, 4),), jnp.float32)
    readout_matrix = gaussian(key_list[6], (2, GROUPS, GROUP_CH, STATE), (2 * STATE) ** -0.5, 0.5, ((1, 4),), jnp.float32)
    skip = gaussian(key_list[7], (MIXER_CHANNELS,), 1.0, 6.0, ((0, 4),), jnp.float32)
    out_proj = gaussian(key_list[8], (MIXER_CHANNELS, D), MIXER_CHANNELS ** -0.5, 0.1875, ((0, 4),))
    stream = gaussian(key_list[9], (SEQ, D), 1.0, 6.0, ((0, 32),))
    norm_gain = jnp.clip(1.0 + 0.18 * jax.random.normal(key_list[10], (D,), jnp.float32), 0.1, 1.9)
    routes_keys = jax.random.split(jax.random.fold_in(key_list[11], 1), SEQ // TOK_DEV)
    routes_turns = jax.random.permutation(jax.random.fold_in(key_list[11], 3), SEQ // TOK_DEV)
    routes = jax.vmap(lambda own, number: assign_block(jax.random.fold_in(key_list[11], 2), own, number, TOK_DEV, EXPERTS, TOP, CAP, 2))(routes_keys, routes_turns).reshape((SEQ, TOP))
    route_logits = draw_route_logits(jax.random.fold_in(key_list[16], 71), 0)
    w_gate = gaussian(key_list[13], (EXPERTS, D, EXPERT_FF), D ** -0.5, 0.125, ((0, 8), (2, 4)))
    w_up = gaussian(key_list[14], (EXPERTS, D, EXPERT_FF), D ** -0.5, 0.125, ((0, 8), (2, 4)))
    w_down = gaussian(key_list[15], (EXPERTS, EXPERT_FF, D), (EXPERT_FF // 9) ** -0.5, 0.21875, ((0, 8), (1, 4)))
    return dict(mixer_input=mixer_input, decay_shift=decay_shift, pole_real=pole_real, pole_imaginary=pole_imaginary, log_step=log_step, input_map=input_map, readout_matrix=readout_matrix, skip=skip, out_proj=out_proj, stream=stream, norm_gain=norm_gain, routes=routes, route_logits=route_logits, w_gate=w_gate, w_up=w_up, w_down=w_down)


TOP_PRECISION = lax.Precision.HIGHEST
EPS = 1e-06
SEGMENT = 16

def discretize(pole_real, pole_imaginary, log_step, input_map):
    step = jnp.exp(log_step)[:, None]
    magnitude = jnp.exp(pole_real * step)
    factor_real = magnitude * jnp.cos(pole_imaginary * step)
    factor_imaginary = magnitude * jnp.sin(pole_imaginary * step)
    denominator = pole_real * pole_real + pole_imaginary * pole_imaginary
    ratio_real = ((factor_real - 1.0) * pole_real + factor_imaginary * pole_imaginary) / denominator
    ratio_imaginary = (factor_imaginary * pole_real - (factor_real - 1.0) * pole_imaginary) / denominator
    map_real = ratio_real[:, :, None] * input_map[0] - ratio_imaginary[:, :, None] * input_map[1]
    map_imaginary = ratio_real[:, :, None] * input_map[1] + ratio_imaginary[:, :, None] * input_map[0]
    return (factor_real, factor_imaginary, map_real, map_imaginary)

def link(earlier, later):
    a_real, a_imag_part, x_real, x_imag_part = earlier
    b_real, b_imag_part, y_real, y_imag_part = later
    return (b_real * a_real - b_imag_part * a_imag_part, b_real * a_imag_part + b_imag_part * a_real, b_real * x_real - b_imag_part * x_imag_part + y_real, b_real * x_imag_part + b_imag_part * x_real + y_imag_part)

def block_states(drive_input, shift, factors):
    factor_real, factor_imaginary, map_real, map_imaginary = factors
    rows, groups = shift.shape
    states = factor_real.shape[1]
    width = groups * states
    grouped = drive_input.reshape(rows, groups, -1)
    drive_real = jnp.einsum('sgc,gpc->sgp', grouped, map_real, precision=TOP_PRECISION).reshape(rows, width)
    drive_imaginary = jnp.einsum('sgc,gpc->sgp', grouped, map_imaginary, precision=TOP_PRECISION).reshape(rows, width)
    scale = jnp.exp(shift)[:, :, None]
    trans_real = (scale * factor_real[None]).reshape(rows, width)
    trans_imaginary = (scale * factor_imaginary[None]).reshape(rows, width)
    segments = rows // SEGMENT

    def arrange(value):
        return jnp.swapaxes(value.reshape(segments, SEGMENT, width), 0, 1)

    def advance(carry, item):
        new = link(carry, item)
        return (new, new)
    first = jnp.ones((segments, width), jnp.float32)
    empty = jnp.zeros((segments, width), jnp.float32)
    _, inner = lax.scan(advance, (first, empty, empty, empty), (arrange(trans_real), arrange(trans_imaginary), arrange(drive_real), arrange(drive_imaginary)))
    totals = tuple((part[-1] for part in inner))
    running = lax.associative_scan(link, totals, axis=0)
    enter = tuple((jnp.concatenate([start, part[:-1]], axis=0) for start, part in zip((first[:1], empty[:1], empty[:1], empty[:1]), running)))
    enter = tuple((part.reshape(segments, width) for part in enter))
    joined = link(tuple((part[None] for part in enter)), inner)

    def restore(value):
        return jnp.swapaxes(value, 0, 1).reshape(rows, groups, states)
    return tuple((restore(part) for part in joined))

def read_out(hidden_state_real, hidden_state_imaginary, readout_matrix):
    return jnp.einsum('ani,nyi->any', hidden_state_real, readout_matrix[0], precision=TOP_PRECISION) - jnp.einsum('ani,nyi->any', hidden_state_imaginary, readout_matrix[1], precision=TOP_PRECISION)

def reference(mixer_input, decay_shift, pole_real, pole_imaginary, log_step, input_map, readout_matrix, skip, out_proj, stream, norm_gain, routes, route_logits, w_gate, w_up, w_down):
    factors = discretize(pole_real, pole_imaginary, log_step, input_map)
    blocks = SEQ // SEQUENCE_LOCAL
    inputs_blocked = mixer_input.astype(jnp.float32).reshape(blocks, SEQUENCE_LOCAL, MIXER_CHANNELS)
    shift_blocked = decay_shift.reshape(blocks, SEQUENCE_LOCAL, GROUPS)

    def advance(carry, pair):
        drive_input, shift = pair
        through_real, through_imaginary, local_real, local_imaginary = block_states(drive_input, shift, factors)
        enter_real, enter_imaginary = carry
        hidden_state_real = local_real + through_real * enter_real[None] - through_imaginary * enter_imaginary[None]
        hidden_state_imaginary = local_imaginary + through_real * enter_imaginary[None] + through_imaginary * enter_real[None]
        response = read_out(hidden_state_real, hidden_state_imaginary, readout_matrix).reshape(SEQUENCE_LOCAL, MIXER_CHANNELS) + skip * drive_input
        activated = jax.nn.gelu(response).astype(jnp.bfloat16)
        return ((hidden_state_real[-1], hidden_state_imaginary[-1]), activated)
    start = (jnp.zeros((GROUPS, STATE), jnp.float32), jnp.zeros((GROUPS, STATE), jnp.float32))
    _, activated = lax.scan(advance, start, (inputs_blocked, shift_blocked))
    projected = jnp.dot(activated.reshape(SEQ, MIXER_CHANNELS), out_proj, preferred_element_type=jnp.float32)
    mixed = (stream.astype(jnp.float32) + projected).astype(jnp.bfloat16)
    mixed_wide = mixed.astype(jnp.float32)
    normed = (mixed_wide * lax.rsqrt(lax.optimization_barrier(jnp.mean(mixed_wide * mixed_wide, axis=-1, keepdims=True)) + EPS) * norm_gain).astype(jnp.bfloat16)
    device_blocks = SEQ // TOK_DEV
    assign = routes.reshape(device_blocks, TOK_DEV * TOP)
    matches = (assign[:, :, None] == jnp.arange(EXPERTS, dtype=jnp.int32)).astype(jnp.int32)
    rank = lax.optimization_barrier(jnp.sum((jnp.cumsum(matches, axis=1) - matches) * matches, axis=2))
    block_ids = jnp.broadcast_to(jnp.arange(device_blocks, dtype=jnp.int32)[:, None], assign.shape)
    token_ids = (jnp.arange(SEQ * TOP, dtype=jnp.int32) // TOP).reshape(device_blocks, TOK_DEV * TOP)
    buffer = jnp.zeros((EXPERTS, device_blocks, CAP, D), jnp.bfloat16)
    buffer = buffer.at[assign, block_ids, rank].set(normed[token_ids])

    def run_expert(pack):
        rows, gate_weight, upward_weight, down_weight = pack
        flat = rows.reshape(device_blocks * CAP, D)
        gate = jnp.dot(flat, gate_weight, preferred_element_type=jnp.float32)
        upward = jnp.dot(flat, upward_weight, preferred_element_type=jnp.float32)
        hidden = (jax.nn.silu(gate) * upward).astype(jnp.bfloat16)
        width = EXPERT_FF // N_TP
        summed = jnp.zeros((device_blocks * CAP, D), jnp.float32)
        for part_index in range(N_TP):
            partial_out = jnp.dot(hidden[:, part_index * width:(part_index + 1) * width], down_weight[part_index * width:(part_index + 1) * width], preferred_element_type=jnp.float32)
            summed = summed + lax.optimization_barrier(partial_out.astype(jnp.bfloat16)).astype(jnp.float32)
        return summed.astype(jnp.bfloat16).reshape(device_blocks, CAP, D)
    outputs = lax.map(run_expert, (buffer, w_gate, w_up, w_down))
    picked = outputs[assign, block_ids, rank].astype(jnp.float32).reshape(SEQ, TOP, D)
    logits = route_logits
    weights = jax.nn.sigmoid(jnp.stack([logits[:, 0] - logits[:, 1], logits[:, 1] - logits[:, 0]], axis=1))
    combined = mixed_wide + lax.optimization_barrier(jnp.sum(picked * weights[:, :, None], axis=1))
    return combined.astype(jnp.bfloat16)
```

```python
import functools

import jax
import jax.numpy as jnp
from jax import lax
from jax.experimental import pallas as pl
from jax.experimental.pallas import tpu as pltpu
from jax.sharding import PartitionSpec as P

TOP_PRECISION = lax.Precision.HIGHEST
EPS = 1e-06
LANES = 8
MESH = pl.DeviceIdType.MESH


def discretize(pole_real, pole_imaginary, log_step, input_map):
    step = jnp.exp(log_step)[:, None]
    magnitude = jnp.exp(pole_real * step)
    factor_real = magnitude * jnp.cos(pole_imaginary * step)
    factor_imaginary = magnitude * jnp.sin(pole_imaginary * step)
    denominator = pole_real * pole_real + pole_imaginary * pole_imaginary
    ratio_real = ((factor_real - 1.0) * pole_real + factor_imaginary * pole_imaginary) / denominator
    ratio_imaginary = (
        factor_imaginary * pole_real - (factor_real - 1.0) * pole_imaginary
    ) / denominator
    map_real = ratio_real[:, :, None] * input_map[0] - ratio_imaginary[:, :, None] * input_map[1]
    map_imaginary = (
        ratio_real[:, :, None] * input_map[1] + ratio_imaginary[:, :, None] * input_map[0]
    )
    return (factor_real, factor_imaginary, map_real, map_imaginary)


def on_ring(body, axis):
    count, mine = lax.axis_size(axis), lax.axis_index(axis)
    barrier = pltpu.get_barrier_semaphore()
    for ahead in range(1, count):
        pl.semaphore_signal(
            barrier,
            inc=1,
            device_id={axis: lax.rem(mine + ahead, count)},
            device_id_type=MESH,
        )
    pl.semaphore_wait(barrier, count - 1)
    body(count, mine)


def exchange_kernel(axis, gather, value, result, send, receive, own):
    def body(count, mine):
        copies = []
        for ahead in range(1, count):
            peer = lax.rem(mine + ahead, count)
            copy = pltpu.make_async_remote_copy(
                src_ref=value if gather else value.at[peer],
                dst_ref=result.at[mine],
                send_sem=send.at[ahead],
                recv_sem=receive.at[ahead],
                device_id={axis: peer},
                device_id_type=MESH,
            )
            copy.start()
            copies.append(copy)
        kept = pltpu.make_async_copy(value if gather else value.at[mine], result.at[mine], own)
        kept.start()
        kept.wait()
        for copy in copies:
            copy.wait()

    on_ring(body, axis)


def exchange(value, axis, number, gather=False):
    count = lax.axis_size(axis)
    shape = ((count,) + value.shape) if gather else value.shape
    return pl.pallas_call(
        functools.partial(exchange_kernel, axis, gather),
        out_shape=jax.ShapeDtypeStruct(shape, value.dtype),
        in_specs=[pl.BlockSpec(memory_space=pltpu.VMEM)],
        out_specs=pl.BlockSpec(memory_space=pltpu.VMEM),
        scratch_shapes=[
            pltpu.SemaphoreType.DMA((count,)),
            pltpu.SemaphoreType.DMA((count,)),
            pltpu.SemaphoreType.DMA,
        ],
        compiler_params=pltpu.CompilerParams(collective_id=number, has_side_effects=True),
        name=f"exchange_{number}",
    )(value)


def across(left, right):
    return lax.dot_general(
        left, right, (((1,), (1,)), ((), ())), preferred_element_type=jnp.float32
    )


def prepare(values, shift, maps, scale, drive_real, drive_imaginary):
    groups, width = shift.shape[1], scale.shape[1]
    spread = lax.broadcasted_iota(jnp.int32, (groups, width), 1) // (width // groups)
    hot = (spread == lax.broadcasted_iota(jnp.int32, (groups, width), 0)).astype(jnp.float32)
    scale[...] = jnp.dot(
        jnp.exp(shift[...]), hot, precision=TOP_PRECISION, preferred_element_type=jnp.float32
    )
    entries = values[...]
    drive_real[...] = across(entries, maps[0]) + across(entries, maps[1])
    drive_imaginary[...] = across(entries, maps[2]) + across(entries, maps[3])


def totals_kernel(values, shift, factor, maps, parts, total, scale, drive_real, drive_imaginary):
    prepare(values, shift, maps, scale, drive_real, drive_imaginary)
    width = scale.shape[1]
    wide = (LANES, width)
    factor_real = jnp.broadcast_to(factor[0:1, :], wide)
    factor_imaginary = jnp.broadcast_to(factor[1:2, :], wide)

    def step(position, carry):
        a_real, a_imaginary, x_real, x_imaginary = carry
        rows = pl.ds(pl.multiple_of(position * LANES, LANES), LANES)
        grow = scale[rows, :]
        b_real, b_imaginary = grow * factor_real, grow * factor_imaginary
        return (
            b_real * a_real - b_imaginary * a_imaginary,
            b_real * a_imaginary + b_imaginary * a_real,
            b_real * x_real - b_imaginary * x_imaginary + drive_real[rows, :],
            b_real * x_imaginary + b_imaginary * x_real + drive_imaginary[rows, :],
        )

    empty = jnp.zeros(wide, jnp.float32)
    ends = lax.fori_loop(
        0, scale.shape[0] // LANES, step, (jnp.ones(wide, jnp.float32), empty, empty, empty)
    )
    for place, end in enumerate(ends):
        parts[place] = end
    run = tuple(end[0:1] for end in ends)
    for segment in range(1, LANES):
        b_real, b_imaginary, y_real, y_imaginary = (
            end[segment : segment + 1] for end in ends
        )
        a_real, a_imaginary, x_real, x_imaginary = run
        run = (
            b_real * a_real - b_imaginary * a_imaginary,
            b_real * a_imaginary + b_imaginary * a_real,
            b_real * x_real - b_imaginary * x_imaginary + y_real,
            b_real * x_imaginary + b_imaginary * x_real + y_imaginary,
        )
    total[...] = jnp.concatenate(run + (jnp.zeros((LANES - 4, width), jnp.float32),), axis=0)


def split(value):
    high = value.astype(jnp.bfloat16)
    return high, (value - high.astype(jnp.float32)).astype(jnp.bfloat16)


def respond_kernel(
    axis, values, shift, factor, maps, parts, gathered, reads, skip, out,
    scale, drive_real, drive_imaginary,
):
    prepare(values, shift, maps, scale, drive_real, drive_imaginary)
    width = scale.shape[1]
    mine = lax.axis_index(axis)

    def before(position, carry):
        real, imaginary = carry
        item = gathered[position]
        a_real, a_imaginary = item[0:1], item[1:2]
        keep = position < mine
        return (
            jnp.where(keep, a_real * real - a_imaginary * imaginary + item[2:3], real),
            jnp.where(keep, a_real * imaginary + a_imaginary * real + item[3:4], imaginary),
        )

    none = jnp.zeros((1, width), jnp.float32)
    real, imaginary = lax.fori_loop(0, gathered.shape[0] - 1, before, (none, none))
    reals, imaginaries = [real], [imaginary]
    for segment in range(LANES - 1):
        at = slice(segment, segment + 1)
        a_real, a_imaginary = parts[0, at, :], parts[1, at, :]
        real, imaginary = (
            a_real * real - a_imaginary * imaginary + parts[2, at, :],
            a_real * imaginary + a_imaginary * real + parts[3, at, :],
        )
        reals.append(real)
        imaginaries.append(imaginary)
    wide = (LANES, width)
    factor_real = jnp.broadcast_to(factor[0:1, :], wide)
    factor_imaginary = jnp.broadcast_to(factor[1:2, :], wide)

    def step(position, carry):
        x_real, x_imaginary = carry
        rows = pl.ds(pl.multiple_of(position * LANES, LANES), LANES)
        grow = scale[rows, :]
        b_real, b_imaginary = grow * factor_real, grow * factor_imaginary
        new_real = b_real * x_real - b_imaginary * x_imaginary + drive_real[rows, :]
        new_imaginary = b_real * x_imaginary + b_imaginary * x_real + drive_imaginary[rows, :]
        drive_real[rows, :] = new_real
        drive_imaginary[rows, :] = new_imaginary
        return new_real, new_imaginary

    lax.fori_loop(
        0,
        scale.shape[0] // LANES,
        step,
        (jnp.concatenate(reals, axis=0), jnp.concatenate(imaginaries, axis=0)),
    )
    high, low = split(drive_real[...])
    response = across(high, reads[0]) + across(low, reads[0]) + across(high, reads[1])
    high, low = split(drive_imaginary[...])
    response -= across(high, reads[2]) + across(low, reads[2]) + across(high, reads[3])
    response += skip[...] * values[...].astype(jnp.float32)
    out[...] = jax.nn.gelu(response).astype(jnp.bfloat16)


def diagonal(blocks):
    groups, rows, columns = blocks.shape
    tiled = jnp.tile(blocks.reshape(groups * rows, columns), (1, groups))
    row = lax.broadcasted_iota(jnp.int32, tiled.shape, 0) // rows
    column = lax.broadcasted_iota(jnp.int32, tiled.shape, 1) // columns
    return split(jnp.where(row == column, tiled, 0.0))


def mixer(mixer_input, decay_shift, factors, readout_matrix, skip):
    factor_real, factor_imaginary, map_real, map_imaginary = factors
    rows, channels = mixer_input.shape
    groups, states = factor_real.shape
    width = groups * states

    def arrange(value):
        return jnp.swapaxes(value.reshape(LANES, rows // LANES, -1), 0, 1).reshape(rows, -1)

    values, shift = arrange(mixer_input), arrange(decay_shift)
    factor = jnp.stack([factor_real.reshape(width), factor_imaginary.reshape(width)])
    maps = jnp.stack(diagonal(map_real) + diagonal(map_imaginary))
    reads = jnp.stack(
        diagonal(readout_matrix[0]) + diagonal(readout_matrix[1])
    )
    vmem = pl.BlockSpec(memory_space=pltpu.VMEM)
    scratch = [pltpu.VMEM((rows, width), jnp.float32)] * 3
    parts, total = pl.pallas_call(
        totals_kernel,
        out_shape=(
            jax.ShapeDtypeStruct((4, LANES, width), jnp.float32),
            jax.ShapeDtypeStruct((LANES, width), jnp.float32),
        ),
        in_specs=[vmem] * 4,
        out_specs=(vmem, vmem),
        scratch_shapes=scratch,
        name="totals",
    )(values, shift, factor, maps)
    gathered = exchange(total, "sp", 0, gather=True)
    activated = pl.pallas_call(
        functools.partial(respond_kernel, "sp"),
        out_shape=jax.ShapeDtypeStruct((rows, channels), jnp.bfloat16),
        in_specs=[vmem] * 8,
        out_specs=vmem,
        scratch_shapes=scratch,
        name="respond",
    )(values, shift, factor, maps, parts, gathered, reads, skip.reshape(1, -1))
    return jnp.swapaxes(activated.reshape(rows // LANES, LANES, channels), 0, 1)


def slot_numbers(route_rows, experts, capacity):
    flat = route_rows.reshape(route_rows.shape[:-2] + (-1,))
    matches = (flat[..., None] == jnp.arange(experts, dtype=jnp.int32)).astype(jnp.int32)
    earlier = jnp.cumsum(matches, axis=-2) - matches
    return flat * capacity + jnp.sum(earlier * matches, axis=-1)


def dispatch_rows(slots, normed, width):
    hits = (slots[..., None] == jnp.arange(width, dtype=jnp.int32)).astype(jnp.bfloat16)
    tokens = normed.shape[-2]
    hits = hits.reshape(slots.shape[:-1] + (tokens, -1, width)).sum(axis=-2)
    return jnp.einsum(
        "...tw,...td->...wd", hits, normed, preferred_element_type=jnp.float32
    ).astype(jnp.bfloat16)


def flip(index, bits):
    bit = 1
    while bit <= bits:
        if bits & bit:
            index = index + bit - 2 * bit * (index // bit % 2)
        bit *= 2
    return index


def shuffle(chunks):
    return [chunk for chunk in range(chunks) if chunk != 1] + [1] if chunks > 1 else [0]


def moe_kernel(
    normed, mixed, routes, weights, w_gate, w_up, w_down, out,
    gate, up, down, outgoing, rows, hidden, kept, given, from_core, to_y, from_y, back, returned,
    load_sem, sp_send, sp_recv, y_send, y_recv, core_send, core_recv, far_send, far_recv,
    rc_send, rc_recv, ry_send, ry_recv, rs_send, rs_recv,
):
    experts = sp_send.shape[0]
    tokens, model = out.shape
    capacity = outgoing.shape[0] // experts
    chunks = rows.shape[0]
    width = gate.shape[1]
    place, share = lax.axis_index("sp"), lax.axis_index("tp")
    partner, across_y = flip(share, 1), flip(share, 2)
    tile, wide = 256, 512
    started = []

    loads = []
    for step in range(width // tile):
        columns = pl.ds(step * tile, tile)
        for number, (source, target) in enumerate(((w_gate, gate), (w_up, up))):
            loads.append(
                pltpu.make_async_copy(
                    source.at[:, columns], target.at[:, columns], load_sem.at[number, step]
                )
            )
    for step in range(model // wide):
        columns = pl.ds(step * wide, wide)
        loads.append(
            pltpu.make_async_copy(w_down.at[:, columns], down.at[:, columns], load_sem.at[2, step])
        )
    for load in loads:
        load.start()

    barrier = pltpu.get_barrier_semaphore()
    for bits in range(1, experts):
        pl.semaphore_signal(
            barrier, inc=1, device_id={"sp": flip(place, bits)}, device_id_type=MESH
        )
    for peer in (partner, across_y):
        pl.semaphore_signal(barrier, inc=1, device_id={"tp": peer}, device_id_type=MESH)

    names = [flip(place, bits) for bits in range(experts)]
    first, second = routes[0:1, :], routes[1:2, :]
    named = jnp.concatenate(
        [((first == name) | (second == name)).astype(jnp.float32) for name in names], axis=0
    )
    earlier = (
        lax.broadcasted_iota(jnp.int32, (tokens, tokens), 0)
        < lax.broadcasted_iota(jnp.int32, (tokens, tokens), 1)
    ).astype(jnp.float32)
    rank = jnp.dot(named, earlier, preferred_element_type=jnp.float32).astype(jnp.int32)
    scale = jnp.concatenate(
        [
            jnp.where(first == name, weights[0:1, :], 0.0)
            + jnp.where(second == name, weights[1:2, :], 0.0)
            for name in names
        ],
        axis=0,
    )
    slot = lax.broadcasted_iota(jnp.int32, (capacity, tokens), 0)
    hits = [
        jnp.where(slot == rank[e : e + 1, :], named[e : e + 1, :], 0.0) for e in range(experts)
    ]
    combine = jnp.concatenate([hit * scale[e : e + 1, :] for e, hit in enumerate(hits)], axis=0)
    outgoing[...] = jnp.dot(
        jnp.concatenate(hits, axis=0).astype(jnp.bfloat16),
        normed[...],
        preferred_element_type=jnp.float32,
    ).astype(jnp.bfloat16)
    spot = (0, 2, 1, 3)

    def at(bits, kind):
        return rows.at[bits // 2, pl.ds((spot[kind] * 2 + bits % 2) * capacity, capacity)]

    def remote(source, target, send, receive, peer):
        copy = pltpu.make_async_remote_copy(
            src_ref=source, dst_ref=target, send_sem=send, recv_sem=receive,
            device_id=peer, device_id_type=MESH,
        )
        copy.start()
        started.append(copy)
        return copy

    def mine(bits):
        return outgoing.at[pl.ds(bits * capacity, capacity)]

    pl.semaphore_wait(barrier, experts + 1)
    arrivals, y_arrivals, core_arrivals, far_arrivals = {}, {}, {}, {}

    def pass_on(bits):
        source = mine(0) if bits == 0 else at(bits, 0)
        y_arrivals[bits] = remote(
            source, at(bits, 2), y_send.at[bits], y_recv.at[bits], {"tp": across_y}
        )
        core_arrivals[bits] = remote(
            source, at(bits, 1), core_send.at[bits], core_recv.at[bits], {"tp": partner}
        )

    pass_on(0)
    order = shuffle(chunks)
    for chunk in order:
        for bits in (2 * chunk, 2 * chunk + 1):
            if bits:
                arrivals[bits] = remote(
                    mine(bits), at(bits, 0), sp_send.at[bits], sp_recv.at[bits],
                    {"sp": names[bits]},
                )
    rows[0, 0:capacity, :] = outgoing[0:capacity, :]

    def relay(chunk):
        for bits in (2 * chunk, 2 * chunk + 1):
            if bits:
                arrivals[bits].wait_recv()
                pass_on(bits)

    def relay_far(chunk):
        for bits in (2 * chunk, 2 * chunk + 1):
            y_arrivals[bits].wait_recv()
            far_arrivals[bits] = remote(
                at(bits, 2), at(bits, 3), far_send.at[bits], far_recv.at[bits], {"tp": partner}
            )

    def ready(chunk):
        for bits in (2 * chunk, 2 * chunk + 1):
            core_arrivals[bits].wait_recv()
            far_arrivals[bits].wait_recv()

    def widen(chunk, low, high, load):
        def body(step, carry):
            columns = pl.ds(pl.multiple_of(step * tile, tile), tile)
            if load:
                for number, (source, target) in enumerate(((w_gate, gate), (w_up, up))):
                    pltpu.make_async_copy(
                        source.at[:, columns], target.at[:, columns], load_sem.at[number, step]
                    ).wait()
            value = rows[chunk]
            opened = jnp.dot(value, gate[:, columns], preferred_element_type=jnp.float32)
            raised = jnp.dot(value, up[:, columns], preferred_element_type=jnp.float32)
            hidden[:, columns] = (jax.nn.silu(opened) * raised).astype(jnp.bfloat16)
            return carry

        lax.fori_loop(low, high, body, 0)

    half = rows.shape[1] // 2
    quarter = half // 2

    def narrow(chunk, load):
        def body(step, carry):
            columns = pl.ds(pl.multiple_of(step * wide, wide), wide)
            if load:
                pltpu.make_async_copy(
                    w_down.at[:, columns], down.at[:, columns], load_sem.at[2, step]
                ).wait()
            value = jnp.dot(hidden[...], down[:, columns], preferred_element_type=jnp.float32)
            kept[chunk, :, columns] = value[:half]
            given[chunk, :, columns] = value[half:].astype(jnp.bfloat16)
            return carry

        lax.fori_loop(0, model // wide, body, 0)

    core_back, y_back, sp_back = {}, {}, {}

    def give(chunk):
        core_back[chunk] = remote(
            given.at[chunk], from_core.at[chunk], rc_send.at[chunk], rc_recv.at[chunk],
            {"tp": partner},
        )

    def cross(chunk):
        core_back[chunk].wait_recv()
        to_y[chunk] = (
            kept[chunk, quarter:, :] + from_core[chunk, quarter:, :].astype(jnp.float32)
        ).astype(jnp.bfloat16)
        y_back[chunk] = remote(
            to_y.at[chunk], from_y.at[chunk], ry_send.at[chunk], ry_recv.at[chunk],
            {"tp": across_y},
        )

    def give_back(chunk):
        y_back[chunk].wait_recv()
        total = (
            kept[chunk, :quarter, :]
            + from_core[chunk, :quarter, :].astype(jnp.float32)
            + from_y[chunk].astype(jnp.float32)
        ).astype(jnp.bfloat16)
        back[chunk] = total
        for side in range(2):
            bits = 2 * chunk + side
            span = pl.ds(side * capacity, capacity)
            if bits:
                sp_back[bits] = remote(
                    back.at[chunk, span], returned.at[pl.ds(bits * capacity, capacity)],
                    rs_send.at[bits], rs_recv.at[bits], {"sp": names[bits]},
                )
            else:
                returned[0:capacity, :] = total[:capacity]

    relay(0)
    relay_far(0)
    ready(0)
    steps = width // tile
    middle = (steps + 1) // 2
    for number, chunk in enumerate(order):
        later = order[number + 1] if number + 1 < chunks else None
        before = order[number - 1] if number else None
        widen(chunk, 0, middle, number == 0)
        if later is not None:
            relay(later)
        if before is not None:
            cross(before)
        widen(chunk, middle, steps, number == 0)
        if later is not None:
            relay_far(later)
        if before is not None:
            give_back(before)
        narrow(chunk, number == 0)
        give(chunk)
        if later is not None:
            ready(later)
    cross(order[-1])
    give_back(order[-1])
    for bits in range(1, experts):
        sp_back[bits].wait_recv()
    high, low = split(combine)
    total = mixed[...].astype(jnp.float32)
    for piece in (high, low):
        total += lax.dot_general(
            piece, returned[...], (((0,), (0,)), ((), ())), preferred_element_type=jnp.float32
        )
    out[...] = total.astype(jnp.bfloat16)
    for copy in started:
        copy.wait_send()


def fits(shares, experts, capacity, w_gate):
    if shares != 4 or w_gate.shape[0] != 1 or experts % 2 or experts & (experts - 1):
        return False
    return capacity % 16 == 0 and w_gate.shape[2] % 256 == 0 and w_gate.shape[1] % 512 == 0


def moe(normed, mixed, routes, weights, w_gate, w_up, w_down, number):
    tokens, model = normed.shape
    experts, shares = lax.axis_size("sp"), lax.axis_size("tp")
    capacity = 4 * tokens // experts
    width = w_gate.shape[1]
    slots, chunks = experts * capacity, experts // 2
    group = 2 * shares * capacity
    bf16, f32 = jnp.bfloat16, jnp.float32
    vmem, anywhere = pl.BlockSpec(memory_space=pltpu.VMEM), pl.BlockSpec(memory_space=pl.ANY)
    steps = max(width // 256, model // 512)
    dma = pltpu.SemaphoreType.DMA
    return pl.pallas_call(
        moe_kernel,
        out_shape=jax.ShapeDtypeStruct((tokens, model), bf16),
        in_specs=[vmem] * 4 + [anywhere] * 3,
        out_specs=vmem,
        scratch_shapes=[
            pltpu.VMEM((model, width), bf16),
            pltpu.VMEM((model, width), bf16),
            pltpu.VMEM((width, model), bf16),
            pltpu.VMEM((slots, model), bf16),
            pltpu.VMEM((chunks, group, model), bf16),
            pltpu.VMEM((group, width), bf16),
            pltpu.VMEM((chunks, group // 2, model), f32),
            pltpu.VMEM((chunks, group // 2, model), bf16),
            pltpu.VMEM((chunks, group // 2, model), bf16),
            pltpu.VMEM((chunks, group // 4, model), bf16),
            pltpu.VMEM((chunks, group // 4, model), bf16),
            pltpu.VMEM((chunks, group // 4, model), bf16),
            pltpu.VMEM((slots, model), bf16),
            dma((3, steps)),
        ]
        + [dma((experts,))] * 8
        + [dma((chunks,))] * 4
        + [dma((experts,))] * 2,
        compiler_params=pltpu.CompilerParams(
            collective_id=number, has_side_effects=True, vmem_limit_bytes=62 * 2**20
        ),
        name="experts",
    )(normed, mixed, routes, weights, w_gate, w_up, w_down)


def shards(
    mixer_input,
    decay_shift,
    pole_real,
    pole_imaginary,
    log_step,
    input_map,
    readout_matrix,
    skip,
    out_proj,
    stream,
    norm_gain,
    routes,
    route_logits,
    w_gate,
    w_up,
    w_down,
):
    factors = discretize(pole_real, pole_imaginary, log_step, input_map)
    shares = lax.axis_size("tp")
    own_rows = stream.shape[0]
    activated = mixer(mixer_input, decay_shift, factors, readout_matrix, skip)
    whole_proj = lax.all_gather(out_proj, "tp", axis=0, tiled=True)
    received = exchange(activated.reshape(shares, own_rows, -1), "tp", 1)
    own_activated = jnp.swapaxes(received, 0, 1).reshape(own_rows, -1)
    projected = jnp.dot(own_activated, whole_proj, preferred_element_type=jnp.float32)
    mixed = (stream.astype(jnp.float32) + projected).astype(jnp.bfloat16)
    mixed_wide = mixed.astype(jnp.float32)
    normed = (
        mixed_wide
        * lax.rsqrt(jnp.mean(mixed_wide * mixed_wide, axis=-1, keepdims=True) + EPS)
        * norm_gain
    ).astype(jnp.bfloat16)
    weights = jax.nn.sigmoid(
        jnp.stack(
            [route_logits[:, 0] - route_logits[:, 1], route_logits[:, 1] - route_logits[:, 0]],
            axis=1,
        )
    )
    experts = lax.axis_size("sp") * w_gate.shape[0]
    capacity = 4 * own_rows // experts
    if fits(shares, experts, capacity, w_gate):
        return moe(
            normed, mixed, routes.T, weights.T, w_gate[0], w_up[0], w_down[0], 2
        )
    slot_width = experts * capacity
    model = stream.shape[1]
    own_slots = slot_numbers(routes, experts, capacity)
    outgoing = dispatch_rows(own_slots, normed, slot_width)
    arrived = exchange(outgoing.reshape(experts, capacity, model), "sp", 2)
    expert_rows = lax.all_gather(arrived.reshape(-1, model), "tp", axis=0, tiled=True)
    gate = jnp.dot(expert_rows, w_gate[0], preferred_element_type=jnp.float32)
    upward = jnp.dot(expert_rows, w_up[0], preferred_element_type=jnp.float32)
    hidden = (jax.nn.silu(gate) * upward).astype(jnp.bfloat16)
    summed = lax.psum_scatter(
        jnp.dot(hidden, w_down[0], preferred_element_type=jnp.float32).astype(jnp.bfloat16),
        "tp",
        scatter_dimension=0,
        tiled=True,
    )
    expert_out = summed.reshape(-1, capacity, model)
    returned_result = exchange(expert_out, "sp", 3).reshape(slot_width, model)
    picked = (
        jnp.take(returned_result, own_slots, axis=0)
        .astype(jnp.float32)
        .reshape(own_rows, -1, model)
    )
    combined = mixed_wide + jnp.sum(picked * weights[:, :, None], axis=1)
    return combined.astype(jnp.bfloat16)


def solution(mesh):
    return jax.shard_map(
        shards,
        mesh=mesh,
        in_specs=(
            P("sp", "tp"),
            P("sp", "tp"),
            P("tp", None),
            P("tp", None),
            P("tp"),
            P(None, "tp", None, None),
            P(None, "tp", None, None),
            P("tp"),
            P("tp", None),
            P(("sp", "tp"), None),
            P(),
            P(("sp", "tp"), None),
            P(("sp", "tp"), None),
            P("sp", None, "tp"),
            P("sp", None, "tp"),
            P("sp", "tp", None),
        ),
        out_specs=P(("sp", "tp"), None),
        check_vma=False,
    )
```

```python
import functools

import jax
import jax.numpy as jnp
from jax import lax
from jax.experimental import pallas as pl
from jax.experimental.pallas import tpu as pltpu
from jax.sharding import PartitionSpec as P

TOP_PRECISION = lax.Precision.HIGHEST
EPS = 1e-06
LANES = 8
MESH = pl.DeviceIdType.MESH


def discretize(pole_real, pole_imaginary, log_step, input_map):
    step = jnp.exp(log_step)[:, None]
    magnitude = jnp.exp(pole_real * step)
    factor_real = magnitude * jnp.cos(pole_imaginary * step)
    factor_imaginary = magnitude * jnp.sin(pole_imaginary * step)
    denominator = pole_real * pole_real + pole_imaginary * pole_imaginary
    ratio_real = ((factor_real - 1.0) * pole_real + factor_imaginary * pole_imaginary) / denominator
    ratio_imaginary = (
        factor_imaginary * pole_real - (factor_real - 1.0) * pole_imaginary
    ) / denominator
    map_real = ratio_real[:, :, None] * input_map[0] - ratio_imaginary[:, :, None] * input_map[1]
    map_imaginary = (
        ratio_real[:, :, None] * input_map[1] + ratio_imaginary[:, :, None] * input_map[0]
    )
    return (factor_real, factor_imaginary, map_real, map_imaginary)


def on_ring(body, axis):
    count, mine = lax.axis_size(axis), lax.axis_index(axis)
    barrier = pltpu.get_barrier_semaphore()
    for ahead in range(1, count):
        pl.semaphore_signal(
            barrier,
            inc=1,
            device_id={axis: lax.rem(mine + ahead, count)},
            device_id_type=MESH,
        )
    pl.semaphore_wait(barrier, count - 1)
    body(count, mine)


def exchange_kernel(axis, gather, value, result, send, receive, own):
    def body(count, mine):
        copies = []
        for ahead in range(1, count):
            peer = lax.rem(mine + ahead, count)
            copy = pltpu.make_async_remote_copy(
                src_ref=value if gather else value.at[peer],
                dst_ref=result.at[mine],
                send_sem=send.at[ahead],
                recv_sem=receive.at[ahead],
                device_id={axis: peer},
                device_id_type=MESH,
            )
            copy.start()
            copies.append(copy)
        kept = pltpu.make_async_copy(value if gather else value.at[mine], result.at[mine], own)
        kept.start()
        kept.wait()
        for copy in copies:
            copy.wait()

    on_ring(body, axis)


def exchange(value, axis, number, gather=False):
    count = lax.axis_size(axis)
    shape = ((count,) + value.shape) if gather else value.shape
    return pl.pallas_call(
        functools.partial(exchange_kernel, axis, gather),
        out_shape=jax.ShapeDtypeStruct(shape, value.dtype),
        in_specs=[pl.BlockSpec(memory_space=pltpu.VMEM)],
        out_specs=pl.BlockSpec(memory_space=pltpu.VMEM),
        scratch_shapes=[
            pltpu.SemaphoreType.DMA((count,)),
            pltpu.SemaphoreType.DMA((count,)),
            pltpu.SemaphoreType.DMA,
        ],
        compiler_params=pltpu.CompilerParams(collective_id=number, has_side_effects=True),
        name=f"exchange_{number}",
    )(value)


def across(left, right):
    return lax.dot_general(
        left, right, (((1,), (1,)), ((), ())), preferred_element_type=jnp.float32
    )


def prepare(values, shift, maps, scale, drive_real, drive_imaginary):
    groups, width = shift.shape[1], scale.shape[1]
    spread = lax.broadcasted_iota(jnp.int32, (groups, width), 1) // (width // groups)
    hot = (spread == lax.broadcasted_iota(jnp.int32, (groups, width), 0)).astype(jnp.float32)
    scale[...] = jnp.dot(
        jnp.exp(shift[...]), hot, precision=TOP_PRECISION, preferred_element_type=jnp.float32
    )
    entries = values[...]
    drive_real[...] = across(entries, maps[0]) + across(entries, maps[1])
    drive_imaginary[...] = across(entries, maps[2]) + across(entries, maps[3])


def totals_kernel(values, shift, factor, maps, parts, total, scale, drive_real, drive_imaginary):
    prepare(values, shift, maps, scale, drive_real, drive_imaginary)
    width = scale.shape[1]
    wide = (LANES, width)
    factor_real = jnp.broadcast_to(factor[0:1, :], wide)
    factor_imaginary = jnp.broadcast_to(factor[1:2, :], wide)

    def step(position, carry):
        a_real, a_imaginary, x_real, x_imaginary = carry
        rows = pl.ds(pl.multiple_of(position * LANES, LANES), LANES)
        grow = scale[rows, :]
        b_real, b_imaginary = grow * factor_real, grow * factor_imaginary
        return (
            b_real * a_real - b_imaginary * a_imaginary,
            b_real * a_imaginary + b_imaginary * a_real,
            b_real * x_real - b_imaginary * x_imaginary + drive_real[rows, :],
            b_real * x_imaginary + b_imaginary * x_real + drive_imaginary[rows, :],
        )

    empty = jnp.zeros(wide, jnp.float32)
    ends = lax.fori_loop(
        0, scale.shape[0] // LANES, step, (jnp.ones(wide, jnp.float32), empty, empty, empty)
    )
    for place, end in enumerate(ends):
        parts[place] = end
    run = tuple(end[0:1] for end in ends)
    for segment in range(1, LANES):
        b_real, b_imaginary, y_real, y_imaginary = (
            end[segment : segment + 1] for end in ends
        )
        a_real, a_imaginary, x_real, x_imaginary = run
        run = (
            b_real * a_real - b_imaginary * a_imaginary,
            b_real * a_imaginary + b_imaginary * a_real,
            b_real * x_real - b_imaginary * x_imaginary + y_real,
            b_real * x_imaginary + b_imaginary * x_real + y_imaginary,
        )
    total[...] = jnp.concatenate(run + (jnp.zeros((LANES - 4, width), jnp.float32),), axis=0)


def split(value):
    high = value.astype(jnp.bfloat16)
    return high, (value - high.astype(jnp.float32)).astype(jnp.bfloat16)


def respond_kernel(
    axis, values, shift, factor, maps, parts, gathered, reads, skip, out,
    scale, drive_real, drive_imaginary,
):
    prepare(values, shift, maps, scale, drive_real, drive_imaginary)
    width = scale.shape[1]
    mine = lax.axis_index(axis)

    def before(position, carry):
        real, imaginary = carry
        item = gathered[position]
        a_real, a_imaginary = item[0:1], item[1:2]
        keep = position < mine
        return (
            jnp.where(keep, a_real * real - a_imaginary * imaginary + item[2:3], real),
            jnp.where(keep, a_real * imaginary + a_imaginary * real + item[3:4], imaginary),
        )

    none = jnp.zeros((1, width), jnp.float32)
    real, imaginary = lax.fori_loop(0, gathered.shape[0] - 1, before, (none, none))
    reals, imaginaries = [real], [imaginary]
    for segment in range(LANES - 1):
        at = slice(segment, segment + 1)
        a_real, a_imaginary = parts[0, at, :], parts[1, at, :]
        real, imaginary = (
            a_real * real - a_imaginary * imaginary + parts[2, at, :],
            a_real * imaginary + a_imaginary * real + parts[3, at, :],
        )
        reals.append(real)
        imaginaries.append(imaginary)
    wide = (LANES, width)
    factor_real = jnp.broadcast_to(factor[0:1, :], wide)
    factor_imaginary = jnp.broadcast_to(factor[1:2, :], wide)

    def step(position, carry):
        x_real, x_imaginary = carry
        rows = pl.ds(pl.multiple_of(position * LANES, LANES), LANES)
        grow = scale[rows, :]
        b_real, b_imaginary = grow * factor_real, grow * factor_imaginary
        new_real = b_real * x_real - b_imaginary * x_imaginary + drive_real[rows, :]
        new_imaginary = b_real * x_imaginary + b_imaginary * x_real + drive_imaginary[rows, :]
        drive_real[rows, :] = new_real
        drive_imaginary[rows, :] = new_imaginary
        return new_real, new_imaginary

    lax.fori_loop(
        0,
        scale.shape[0] // LANES,
        step,
        (jnp.concatenate(reals, axis=0), jnp.concatenate(imaginaries, axis=0)),
    )
    high, low = split(drive_real[...])
    response = across(high, reads[0]) + across(low, reads[0]) + across(high, reads[1])
    high, low = split(drive_imaginary[...])
    response -= across(high, reads[2]) + across(low, reads[2]) + across(high, reads[3])
    response += skip[...] * values[...].astype(jnp.float32)
    out[...] = jax.nn.gelu(response).astype(jnp.bfloat16)


def diagonal(blocks):
    groups, rows, columns = blocks.shape
    tiled = jnp.tile(blocks.reshape(groups * rows, columns), (1, groups))
    row = lax.broadcasted_iota(jnp.int32, tiled.shape, 0) // rows
    column = lax.broadcasted_iota(jnp.int32, tiled.shape, 1) // columns
    return split(jnp.where(row == column, tiled, 0.0))


def mixer(mixer_input, decay_shift, factors, readout_matrix, skip):
    factor_real, factor_imaginary, map_real, map_imaginary = factors
    rows, channels = mixer_input.shape
    groups, states = factor_real.shape
    width = groups * states

    def arrange(value):
        return jnp.swapaxes(value.reshape(LANES, rows // LANES, -1), 0, 1).reshape(rows, -1)

    values, shift = arrange(mixer_input), arrange(decay_shift)
    factor = jnp.stack([factor_real.reshape(width), factor_imaginary.reshape(width)])
    maps = jnp.stack(diagonal(map_real) + diagonal(map_imaginary))
    reads = jnp.stack(
        diagonal(readout_matrix[0]) + diagonal(readout_matrix[1])
    )
    vmem = pl.BlockSpec(memory_space=pltpu.VMEM)
    scratch = [pltpu.VMEM((rows, width), jnp.float32)] * 3
    parts, total = pl.pallas_call(
        totals_kernel,
        out_shape=(
            jax.ShapeDtypeStruct((4, LANES, width), jnp.float32),
            jax.ShapeDtypeStruct((LANES, width), jnp.float32),
        ),
        in_specs=[vmem] * 4,
        out_specs=(vmem, vmem),
        scratch_shapes=scratch,
        name="totals",
    )(values, shift, factor, maps)
    gathered = exchange(total, "sp", 0, gather=True)
    activated = pl.pallas_call(
        functools.partial(respond_kernel, "sp"),
        out_shape=jax.ShapeDtypeStruct((rows, channels), jnp.bfloat16),
        in_specs=[vmem] * 8,
        out_specs=vmem,
        scratch_shapes=scratch,
        name="respond",
    )(values, shift, factor, maps, parts, gathered, reads, skip.reshape(1, -1))
    return jnp.swapaxes(activated.reshape(rows // LANES, LANES, channels), 0, 1)


def slot_numbers(route_rows, experts, capacity):
    flat = route_rows.reshape(route_rows.shape[:-2] + (-1,))
    matches = (flat[..., None] == jnp.arange(experts, dtype=jnp.int32)).astype(jnp.int32)
    earlier = jnp.cumsum(matches, axis=-2) - matches
    return flat * capacity + jnp.sum(earlier * matches, axis=-1)


def dispatch_rows(slots, normed, width):
    hits = (slots[..., None] == jnp.arange(width, dtype=jnp.int32)).astype(jnp.bfloat16)
    tokens = normed.shape[-2]
    hits = hits.reshape(slots.shape[:-1] + (tokens, -1, width)).sum(axis=-2)
    return jnp.einsum(
        "...tw,...td->...wd", hits, normed, preferred_element_type=jnp.float32
    ).astype(jnp.bfloat16)


def flip(index, bits):
    bit = 1
    while bit <= bits:
        if bits & bit:
            index = index + bit - 2 * bit * (index // bit % 2)
        bit *= 2
    return index


def plan(experts):
    if experts == 8:
        order, sends = (0, 1, 4, 2, 5, 6, 7, 3), (1, 4, 2, 5, 6, 7, 3)
        near, far = (0, 0, 0, 1, 6, 12, 15, 17), (0, 0, 5, 7, 12, 17, 20, 23)
    else:
        order, sends = tuple(range(experts)), tuple(range(1, experts))
        near = tuple(max(0, 4 * place - 12) for place in range(experts))
        far = tuple(max(0, 4 * place - 6) for place in range(experts))
    events = {slot: [] for slot in range(4 * experts)}
    for place in range(experts):
        if place > 1:
            events[near[place]].append(("pass_on", order[place]))
        if place > 0:
            events[far[place]].append(("pass_far", order[place]))
    late = []
    for place in range(experts):
        for name, slot in (("cross", 4 * place + 5), ("give_back", 4 * place + 10)):
            if slot < 4 * experts:
                events[slot].append((name, order[place]))
            else:
                late.append((slot, name, order[place]))
    return order, sends, events, [item[1:] for item in sorted(late)]


def moe_kernel(
    normed, mixed, routes, weights, w_gate, w_up, w_down, out,
    gate, up, down, outgoing, rows, hidden, kept, given, from_core, to_y, from_y, back, returned,
    load_sem, send_sem, recv_sem,
):
    experts = rows.shape[0]
    tokens, model = out.shape
    capacity = outgoing.shape[1]
    width = gate.shape[1]
    tile, wide = width // 2, model // 2
    place, share = lax.axis_index("sp"), lax.axis_index("tp")
    partner, across_y = flip(share, 1), flip(share, 2)
    names = [flip(place, bits) for bits in range(experts)]
    order, sends, events, late = plan(experts)

    def load(number, step):
        source, target = ((w_gate, gate), (w_up, up), (w_down, down))[number]
        length = wide if number == 2 else tile
        columns = pl.ds(pl.multiple_of(step * length, 128), length)
        return pltpu.make_async_copy(
            source.at[:, columns], target.at[:, columns], load_sem.at[number, step]
        )

    for step in range(2):
        load(0, step).start()
        load(1, step).start()
    for step in range(2):
        load(2, step).start()

    barrier = pltpu.get_barrier_semaphore()
    for bits in range(1, experts):
        pl.semaphore_signal(barrier, inc=1, device_id={"sp": names[bits]}, device_id_type=MESH)
    for peer in (partner, across_y):
        pl.semaphore_signal(barrier, inc=1, device_id={"tp": peer}, device_id_type=MESH)

    first, second = routes[0:1, :], routes[1:2, :]
    named = jnp.concatenate(
        [((first == name) | (second == name)).astype(jnp.float32) for name in names], axis=0
    )
    earlier = (
        lax.broadcasted_iota(jnp.int32, (tokens, tokens), 0)
        < lax.broadcasted_iota(jnp.int32, (tokens, tokens), 1)
    ).astype(jnp.float32)
    rank = jnp.dot(named, earlier, preferred_element_type=jnp.float32).astype(jnp.int32)
    scale = jnp.concatenate(
        [
            jnp.where(first == name, weights[0:1, :], 0.0)
            + jnp.where(second == name, weights[1:2, :], 0.0)
            for name in names
        ],
        axis=0,
    )
    slot = lax.broadcasted_iota(jnp.int32, (capacity, tokens), 0)
    hits = [
        jnp.where(slot == rank[e : e + 1, :], named[e : e + 1, :], 0.0) for e in range(experts)
    ]
    combine = jnp.concatenate([hit * scale[e : e + 1, :] for e, hit in enumerate(hits)], axis=0)
    outgoing[...] = (
        jnp.dot(
            jnp.concatenate(hits, axis=0).astype(jnp.bfloat16),
            normed[...],
            preferred_element_type=jnp.float32,
        )
        .astype(jnp.bfloat16)
        .reshape(outgoing.shape)
    )
    spot = (0, 2, 1, 3)

    def at(bits, kind):
        return rows.at[bits, pl.ds(spot[kind] * capacity, capacity)]

    def remote(kind, bits):
        source, target, peer = {
            "sp": lambda: (outgoing.at[bits], at(bits, 0), {"sp": names[bits]}),
            "y": lambda: (at(bits, 0), at(bits, 2), {"tp": across_y}),
            "core": lambda: (at(bits, 0), at(bits, 1), {"tp": partner}),
            "far": lambda: (at(bits, 2), at(bits, 3), {"tp": partner}),
            "core_back": lambda: (given.at[bits], from_core.at[bits], {"tp": partner}),
            "y_back": lambda: (to_y.at[bits], from_y.at[bits], {"tp": across_y}),
            "sp_back": lambda: (back.at[bits], returned.at[bits], {"sp": names[bits]}),
        }[kind]()
        if bits == 0 and kind in ("y", "core"):
            source = outgoing.at[0]
        number = KINDS.index(kind)
        return pltpu.make_async_remote_copy(
            src_ref=source, dst_ref=target,
            send_sem=send_sem.at[number, bits], recv_sem=recv_sem.at[number, bits],
            device_id=peer, device_id_type=MESH,
        )

    def pass_on(bits):
        if bits:
            remote("sp", bits).wait_recv()
        remote("y", bits).start()
        remote("core", bits).start()

    def pass_far(bits):
        remote("y", bits).wait_recv()
        remote("far", bits).start()

    def cross(bits):
        remote("core_back", bits).wait_recv()
        to_y[bits] = (
            kept[bits, capacity:, :] + from_core[bits, capacity:, :].astype(jnp.float32)
        ).astype(jnp.bfloat16)
        remote("y_back", bits).start()

    def give_back(bits):
        remote("y_back", bits).wait_recv()
        total = (
            kept[bits, :capacity, :]
            + from_core[bits, :capacity, :].astype(jnp.float32)
            + from_y[bits].astype(jnp.float32)
        ).astype(jnp.bfloat16)
        if bits:
            back[bits] = total
            remote("sp_back", bits).start()
        else:
            returned[0] = total

    acts = {"pass_on": pass_on, "pass_far": pass_far, "cross": cross, "give_back": give_back}

    def act(step, slots):
        for number, slot in enumerate(slots):
            if events[slot]:
                @pl.when(step == number)
                def _():
                    for name, bits in events[slot]:
                        acts[name](bits)

    pl.semaphore_wait(barrier, experts + 1)
    pass_on(0)
    for bits in sends:
        remote("sp", bits).start()
    rows[0, 0:capacity, :] = outgoing[0]
    pass_on(order[1])
    pass_far(0)
    for number, bits in enumerate(order):
        remote("core", bits).wait_recv()
        remote("far", bits).wait_recv()

        def widen(step, carry):
            columns = pl.ds(pl.multiple_of(step * tile, 128), tile)
            if number == 0:
                load(0, step).wait()
                load(1, step).wait()
            value = rows[bits]
            opened = jnp.dot(value, gate[:, columns], preferred_element_type=jnp.float32)
            raised = jnp.dot(value, up[:, columns], preferred_element_type=jnp.float32)
            hidden[:, columns] = (jax.nn.silu(opened) * raised).astype(jnp.bfloat16)
            act(step, (4 * number, 4 * number + 1))
            return carry

        lax.fori_loop(0, 2, widen, 0)

        def narrow(step, carry):
            columns = pl.ds(pl.multiple_of(step * wide, 128), wide)
            if number == 0:
                load(2, step).wait()
            value = jnp.dot(hidden[...], down[:, columns], preferred_element_type=jnp.float32)
            kept[bits, :, columns] = value[: 2 * capacity]
            given[bits, :, columns] = value[2 * capacity :].astype(jnp.bfloat16)
            act(step, (4 * number + 2, 4 * number + 3))
            return carry

        lax.fori_loop(0, 2, narrow, 0)
        remote("core_back", bits).start()
    for name, bits in late:
        acts[name](bits)
    for bits in sends:
        remote("sp_back", bits).wait_recv()
    total = mixed[...].astype(jnp.float32)
    every = returned[...].reshape(experts * capacity, model)
    for piece in split(combine):
        total += lax.dot_general(
            piece, every, (((0,), (0,)), ((), ())), preferred_element_type=jnp.float32
        )
    out[...] = total.astype(jnp.bfloat16)
    for bits in range(experts):
        for kind in KINDS:
            if bits or kind not in ("sp", "sp_back"):
                remote(kind, bits).wait_send()


KINDS = ("sp", "y", "core", "far", "core_back", "y_back", "sp_back")


def fits(shares, experts, capacity, w_gate):
    if shares != 4 or w_gate.shape[0] != 1 or experts & (experts - 1) or experts < 2:
        return False
    return capacity % 16 == 0 and w_gate.shape[2] % 256 == 0 and w_gate.shape[1] % 256 == 0


def moe(normed, mixed, routes, weights, w_gate, w_up, w_down, number):
    tokens, model = normed.shape
    experts = lax.axis_size("sp")
    capacity = 4 * tokens // experts
    width = w_gate.shape[1]
    group = 4 * capacity
    bf16, f32 = jnp.bfloat16, jnp.float32
    vmem, anywhere = pl.BlockSpec(memory_space=pltpu.VMEM), pl.BlockSpec(memory_space=pl.ANY)
    dma = pltpu.SemaphoreType.DMA
    return pl.pallas_call(
        moe_kernel,
        out_shape=jax.ShapeDtypeStruct((tokens, model), bf16),
        in_specs=[vmem] * 4 + [anywhere] * 3,
        out_specs=vmem,
        scratch_shapes=[
            pltpu.VMEM((model, width), bf16),
            pltpu.VMEM((model, width), bf16),
            pltpu.VMEM((width, model), bf16),
            pltpu.VMEM((experts, capacity, model), bf16),
            pltpu.VMEM((experts, group, model), bf16),
            pltpu.VMEM((group, width), bf16),
            pltpu.VMEM((experts, 2 * capacity, model), f32),
            pltpu.VMEM((experts, 2 * capacity, model), bf16),
            pltpu.VMEM((experts, 2 * capacity, model), bf16),
            pltpu.VMEM((experts, capacity, model), bf16),
            pltpu.VMEM((experts, capacity, model), bf16),
            pltpu.VMEM((experts, capacity, model), bf16),
            pltpu.VMEM((experts, capacity, model), bf16),
            dma((3, 2)),
            dma((len(KINDS), experts)),
            dma((len(KINDS), experts)),
        ],
        compiler_params=pltpu.CompilerParams(
            collective_id=number, has_side_effects=True, vmem_limit_bytes=62 * 2**20
        ),
        name="experts",
    )(normed, mixed, routes, weights, w_gate, w_up, w_down)


def same(shape, row, column):
    rows = lax.broadcasted_iota(jnp.int32, shape, 0)
    columns = lax.broadcasted_iota(jnp.int32, shape, 1)
    return row(rows) == column(columns)


def chain(later, earlier):
    b_real, b_imaginary, y_real, y_imaginary = later
    a_real, a_imaginary, x_real, x_imaginary = earlier
    return (
        b_real * a_real - b_imaginary * a_imaginary,
        b_real * a_imaginary + b_imaginary * a_real,
        b_real * x_real - b_imaginary * x_imaginary + y_real,
        b_real * x_imaginary + b_imaginary * x_real + y_imaginary,
    )


def mixer_kernel(
    values, shift, pole_real, pole_imaginary, log_step, input_map, readout, skip, out_proj,
    stream, gain, mixed, normed,
    scale, drive_real, drive_imaginary, parts, total, gathered, activated, acts, proj,
    sp_send, sp_recv, tp_send, tp_recv, proj_send, proj_recv,
):
    rows, width = scale.shape
    groups, states = pole_real.shape
    inner = input_map.shape[1]
    channels = groups * inner
    own_rows = mixed.shape[0]
    count = lax.axis_size("sp")
    place, share = lax.axis_index("sp"), lax.axis_index("tp")
    partner, across_y = flip(share, 1), flip(share, 2)
    float_dot = functools.partial(
        jnp.dot, precision=TOP_PRECISION, preferred_element_type=jnp.float32
    )
    pieces = proj_send.shape[1]
    depth = channels // pieces

    barrier = pltpu.get_barrier_semaphore()
    for bits in range(1, count):
        pl.semaphore_signal(
            barrier, inc=1, device_id={"sp": flip(place, bits)}, device_id_type=MESH
        )
    for kind in range(1, 4):
        pl.semaphore_signal(
            barrier, inc=1, device_id={"tp": flip(share, kind)}, device_id_type=MESH
        )

    def remote(source, target, send, receive, peer):
        return pltpu.make_async_remote_copy(
            src_ref=source, dst_ref=target, send_sem=send, recv_sem=receive,
            device_id=peer, device_id_type=MESH,
        )

    def weights(kind, piece):
        span = pl.ds(piece * depth, depth)
        source = proj.at[2, span] if kind == 3 else out_proj.at[span]
        peer = across_y if kind == 2 else partner
        return remote(
            source, proj.at[kind, span], proj_send.at[kind, piece], proj_recv.at[kind, piece],
            {"tp": peer},
        )

    pl.semaphore_wait(barrier, count + 2)
    for piece in range(pieces):
        weights(2, piece).start()
    for piece in range(pieces):
        weights(1, piece).start()

    spread = same((states, width), lambda r: r, lambda c: c % states).astype(jnp.float32)
    group = same((groups, width), lambda r: r, lambda c: c // states)
    stacked = jnp.concatenate(
        [
            pole_real[...],
            pole_imaginary[...],
            jnp.broadcast_to(log_step[...], (groups, states)),
        ],
        axis=0,
    )
    laid = float_dot(stacked, spread)
    real, imaginary, logarithm = (
        jnp.sum(
            jnp.where(group, laid[n * groups : (n + 1) * groups], 0.0), axis=0, keepdims=True
        )
        for n in range(3)
    )
    step = jnp.exp(logarithm)
    magnitude = jnp.exp(real * step)
    factor_real = magnitude * jnp.cos(imaginary * step)
    factor_imaginary = magnitude * jnp.sin(imaginary * step)
    denominator = real * real + imaginary * imaginary
    ratio_real = ((factor_real - 1.0) * real + factor_imaginary * imaginary) / denominator
    ratio_imaginary = (factor_imaginary * real - (factor_real - 1.0) * imaginary) / denominator
    map_real = ratio_real * input_map[0] - ratio_imaginary * input_map[1]
    map_imaginary = ratio_real * input_map[1] + ratio_imaginary * input_map[0]

    segment = rows // LANES
    permute = same((rows, rows), lambda r: r % LANES * segment + r // LANES, lambda c: c)
    entries = jnp.dot(
        permute.astype(jnp.bfloat16), values[...], preferred_element_type=jnp.float32
    ).astype(jnp.bfloat16)
    growth = float_dot(permute.astype(jnp.float32), jnp.exp(shift[...]))
    scale[...] = float_dot(growth, group.astype(jnp.float32))
    block = same((channels, width), lambda r: r // inner, lambda c: c // states)

    def diagonal(value):
        return [
            jnp.where(block, jnp.concatenate([piece] * groups, axis=0), 0.0).astype(jnp.bfloat16)
            for piece in (part.astype(jnp.float32) for part in split(value))
        ]

    for target, value in ((drive_real, map_real), (drive_imaginary, map_imaginary)):
        high, low = diagonal(value)
        target[...] = jnp.dot(entries, high, preferred_element_type=jnp.float32) + jnp.dot(
            entries, low, preferred_element_type=jnp.float32
        )

    wide = (LANES, width)
    wide_real = jnp.broadcast_to(factor_real, wide)
    wide_imaginary = jnp.broadcast_to(factor_imaginary, wide)

    def first_pass(position, carry):
        at = pl.ds(pl.multiple_of(position * LANES, LANES), LANES)
        grow = scale[at, :]
        item = (
            grow * wide_real, grow * wide_imaginary, drive_real[at, :], drive_imaginary[at, :]
        )
        return chain(item, carry)

    empty = jnp.zeros(wide, jnp.float32)
    ends = lax.fori_loop(
        0, segment, first_pass, (jnp.ones(wide, jnp.float32), empty, empty, empty)
    )
    for number, end in enumerate(ends):
        parts[number] = end
    run = tuple(end[0:1] for end in ends)
    for number in range(1, LANES):
        run = chain(tuple(end[number : number + 1] for end in ends), run)
    total[...] = jnp.concatenate(run + (jnp.zeros((LANES - 4, width), jnp.float32),), axis=0)
    gathered[place] = total[...]

    def totals(bits):
        return remote(
            total, gathered.at[place], sp_send.at[bits], sp_recv.at[bits],
            {"sp": flip(place, bits)},
        )

    for bits in range(1, count):
        totals(bits).start()

    spread_low = spread.astype(jnp.bfloat16)
    reads = []
    for number in range(2):
        for piece in split(readout[number]):
            tiled = jnp.dot(piece, spread_low, preferred_element_type=jnp.float32)
            reads.append(jnp.where(block, tiled, 0.0).astype(jnp.bfloat16))
    for bits in range(1, count):
        totals(bits).wait_recv()

    def before(position, carry):
        real, imaginary = carry
        item = gathered[position]
        a_real, a_imaginary = item[0:1], item[1:2]
        keep = position < place
        return (
            jnp.where(keep, a_real * real - a_imaginary * imaginary + item[2:3], real),
            jnp.where(keep, a_real * imaginary + a_imaginary * real + item[3:4], imaginary),
        )

    none = jnp.zeros((1, width), jnp.float32)
    real, imaginary = lax.fori_loop(0, count - 1, before, (none, none))
    reals, imaginaries = [real], [imaginary]
    for number in range(LANES - 1):
        at = slice(number, number + 1)
        a_real, a_imaginary = parts[0, at, :], parts[1, at, :]
        real, imaginary = (
            a_real * real - a_imaginary * imaginary + parts[2, at, :],
            a_real * imaginary + a_imaginary * real + parts[3, at, :],
        )
        reals.append(real)
        imaginaries.append(imaginary)

    def second_pass(position, carry):
        x_real, x_imaginary = carry
        at = pl.ds(pl.multiple_of(position * LANES, LANES), LANES)
        grow = scale[at, :]
        b_real, b_imaginary = grow * wide_real, grow * wide_imaginary
        new_real = b_real * x_real - b_imaginary * x_imaginary + drive_real[at, :]
        new_imaginary = b_real * x_imaginary + b_imaginary * x_real + drive_imaginary[at, :]
        drive_real[at, :] = new_real
        drive_imaginary[at, :] = new_imaginary
        return new_real, new_imaginary

    lax.fori_loop(
        0,
        segment,
        second_pass,
        (jnp.concatenate(reals, axis=0), jnp.concatenate(imaginaries, axis=0)),
    )
    high, low = split(drive_real[...])
    response = across(high, reads[0]) + across(low, reads[0]) + across(high, reads[1])
    high, low = split(drive_imaginary[...])
    response -= across(high, reads[2]) + across(low, reads[2]) + across(high, reads[3])
    response += skip[...] * entries.astype(jnp.float32)
    restore = same((rows, rows), lambda r: r, lambda c: c % LANES * segment + c // LANES)
    activated[...] = jnp.dot(
        restore.astype(jnp.bfloat16),
        jax.nn.gelu(response).astype(jnp.bfloat16),
        preferred_element_type=jnp.float32,
    ).astype(jnp.bfloat16)

    def hand(kind):
        peer = flip(share, kind)
        start = pl.multiple_of(peer * own_rows, own_rows)
        return remote(
            activated.at[pl.ds(start, own_rows)], acts.at[kind], tp_send.at[kind],
            tp_recv.at[kind], {"tp": peer},
        )

    for kind in range(1, 4):
        hand(kind).start()
    acts[0] = activated[pl.ds(pl.multiple_of(share * own_rows, own_rows), own_rows), :]
    for piece in range(pieces):
        weights(2, piece).wait_recv()
        weights(3, piece).start()
    projected = jnp.dot(acts[0], out_proj[...], preferred_element_type=jnp.float32)
    for kind in range(1, 4):
        hand(kind).wait_recv()
        for piece in range(pieces):
            if kind != 2:
                weights(kind, piece).wait_recv()
        projected += jnp.dot(acts[kind], proj[kind], preferred_element_type=jnp.float32)
    result = (stream[...].astype(jnp.float32) + projected).astype(jnp.bfloat16)
    mixed[...] = result
    broad = result.astype(jnp.float32)
    normed[...] = (
        broad * lax.rsqrt(jnp.mean(broad * broad, axis=-1, keepdims=True) + EPS) * gain[...]
    ).astype(jnp.bfloat16)
    for bits in range(1, count):
        totals(bits).wait_send()
    for kind in range(1, 4):
        hand(kind).wait_send()
        for piece in range(pieces):
            weights(kind, piece).wait_send()


def mixer_block(
    mixer_input, decay_shift, pole_real, pole_imaginary, log_step, input_map, readout_matrix,
    skip, out_proj, stream, norm_gain, number,
):
    rows, channels = mixer_input.shape
    groups, states = pole_real.shape
    width = groups * states
    count = lax.axis_size("sp")
    own_rows, model = stream.shape
    bf16, f32 = jnp.bfloat16, jnp.float32
    vmem = pl.BlockSpec(memory_space=pltpu.VMEM)
    dma = pltpu.SemaphoreType.DMA
    pieces = 2
    turned = jnp.swapaxes(input_map.reshape(2, width, -1), 1, 2)
    return pl.pallas_call(
        mixer_kernel,
        out_shape=(jax.ShapeDtypeStruct((own_rows, model), bf16),) * 2,
        in_specs=[vmem] * 11,
        out_specs=(vmem, vmem),
        scratch_shapes=[pltpu.VMEM((rows, width), f32)] * 3
        + [
            pltpu.VMEM((4, LANES, width), f32),
            pltpu.VMEM((LANES, width), f32),
            pltpu.VMEM((count, LANES, width), f32),
            pltpu.VMEM((rows, channels), bf16),
            pltpu.VMEM((4, own_rows, channels), bf16),
            pltpu.VMEM((4, channels, model), bf16),
            dma((count,)),
            dma((count,)),
            dma((4,)),
            dma((4,)),
            dma((4, pieces)),
            dma((4, pieces)),
        ],
        compiler_params=pltpu.CompilerParams(
            collective_id=number, has_side_effects=True, vmem_limit_bytes=48 * 2**20
        ),
        name="mixer",
    )(
        mixer_input, decay_shift, pole_real, pole_imaginary, log_step.reshape(-1, 1), turned,
        readout_matrix.reshape(2, channels, states), skip.reshape(1, -1), out_proj, stream,
        norm_gain.reshape(1, -1),
    )


def shards(
    mixer_input,
    decay_shift,
    pole_real,
    pole_imaginary,
    log_step,
    input_map,
    readout_matrix,
    skip,
    out_proj,
    stream,
    norm_gain,
    routes,
    route_logits,
    w_gate,
    w_up,
    w_down,
):
    shares = lax.axis_size("tp")
    own_rows = stream.shape[0]
    weights = jax.nn.sigmoid(
        jnp.stack(
            [route_logits[:, 0] - route_logits[:, 1], route_logits[:, 1] - route_logits[:, 0]],
            axis=1,
        )
    )
    experts = lax.axis_size("sp") * w_gate.shape[0]
    capacity = 4 * own_rows // experts
    if fits(shares, experts, capacity, w_gate):
        mixed, normed = mixer_block(
            mixer_input, decay_shift, pole_real, pole_imaginary, log_step, input_map,
            readout_matrix, skip, out_proj, stream, norm_gain, 1,
        )
        return moe(normed, mixed, routes.T, weights.T, w_gate[0], w_up[0], w_down[0], 2)
    factors = discretize(pole_real, pole_imaginary, log_step, input_map)
    activated = mixer(mixer_input, decay_shift, factors, readout_matrix, skip)
    whole_proj = lax.all_gather(out_proj, "tp", axis=0, tiled=True)
    received = exchange(activated.reshape(shares, own_rows, -1), "tp", 1)
    own_activated = jnp.swapaxes(received, 0, 1).reshape(own_rows, -1)
    projected = jnp.dot(own_activated, whole_proj, preferred_element_type=jnp.float32)
    mixed = (stream.astype(jnp.float32) + projected).astype(jnp.bfloat16)
    mixed_wide = mixed.astype(jnp.float32)
    normed = (
        mixed_wide
        * lax.rsqrt(jnp.mean(mixed_wide * mixed_wide, axis=-1, keepdims=True) + EPS)
        * norm_gain
    ).astype(jnp.bfloat16)
    slot_width = experts * capacity
    model = stream.shape[1]
    own_slots = slot_numbers(routes, experts, capacity)
    outgoing = dispatch_rows(own_slots, normed, slot_width)
    arrived = exchange(outgoing.reshape(experts, capacity, model), "sp", 2)
    expert_rows = lax.all_gather(arrived.reshape(-1, model), "tp", axis=0, tiled=True)
    gate = jnp.dot(expert_rows, w_gate[0], preferred_element_type=jnp.float32)
    upward = jnp.dot(expert_rows, w_up[0], preferred_element_type=jnp.float32)
    hidden = (jax.nn.silu(gate) * upward).astype(jnp.bfloat16)
    summed = lax.psum_scatter(
        jnp.dot(hidden, w_down[0], preferred_element_type=jnp.float32).astype(jnp.bfloat16),
        "tp",
        scatter_dimension=0,
        tiled=True,
    )
    expert_out = summed.reshape(-1, capacity, model)
    returned_result = exchange(expert_out, "sp", 3).reshape(slot_width, model)
    picked = (
        jnp.take(returned_result, own_slots, axis=0)
        .astype(jnp.float32)
        .reshape(own_rows, -1, model)
    )
    combined = mixed_wide + jnp.sum(picked * weights[:, :, None], axis=1)
    return combined.astype(jnp.bfloat16)


def solution(mesh):
    return jax.shard_map(
        shards,
        mesh=mesh,
        in_specs=(
            P("sp", "tp"),
            P("sp", "tp"),
            P("tp", None),
            P("tp", None),
            P("tp"),
            P(None, "tp", None, None),
            P(None, "tp", None, None),
            P("tp"),
            P("tp", None),
            P(("sp", "tp"), None),
            P(),
            P(("sp", "tp"), None),
            P(("sp", "tp"), None),
            P("sp", None, "tp"),
            P("sp", None, "tp"),
            P("sp", "tp", None),
        ),
        out_specs=P(("sp", "tp"), None),
        check_vma=False,
    )
```

```python
import functools

import jax
import jax.numpy as jnp
from jax import lax
from jax.experimental import pallas as pl
from jax.experimental.pallas import tpu as pltpu
from jax.sharding import PartitionSpec as P

TOP_PRECISION = lax.Precision.HIGHEST
EPS = 1e-06
LANES = 8
MESH = pl.DeviceIdType.MESH


def discretize(pole_real, pole_imaginary, log_step, input_map):
    step = jnp.exp(log_step)[:, None]
    magnitude = jnp.exp(pole_real * step)
    factor_real = magnitude * jnp.cos(pole_imaginary * step)
    factor_imaginary = magnitude * jnp.sin(pole_imaginary * step)
    denominator = pole_real * pole_real + pole_imaginary * pole_imaginary
    ratio_real = ((factor_real - 1.0) * pole_real + factor_imaginary * pole_imaginary) / denominator
    ratio_imaginary = (
        factor_imaginary * pole_real - (factor_real - 1.0) * pole_imaginary
    ) / denominator
    map_real = ratio_real[:, :, None] * input_map[0] - ratio_imaginary[:, :, None] * input_map[1]
    map_imaginary = (
        ratio_real[:, :, None] * input_map[1] + ratio_imaginary[:, :, None] * input_map[0]
    )
    return (factor_real, factor_imaginary, map_real, map_imaginary)


def on_ring(body, axis):
    count, mine = lax.axis_size(axis), lax.axis_index(axis)
    barrier = pltpu.get_barrier_semaphore()
    for ahead in range(1, count):
        pl.semaphore_signal(
            barrier,
            inc=1,
            device_id={axis: lax.rem(mine + ahead, count)},
            device_id_type=MESH,
        )
    pl.semaphore_wait(barrier, count - 1)
    body(count, mine)


def exchange_kernel(axis, gather, value, result, send, receive, own):
    def body(count, mine):
        copies = []
        for ahead in range(1, count):
            peer = lax.rem(mine + ahead, count)
            copy = pltpu.make_async_remote_copy(
                src_ref=value if gather else value.at[peer],
                dst_ref=result.at[mine],
                send_sem=send.at[ahead],
                recv_sem=receive.at[ahead],
                device_id={axis: peer},
                device_id_type=MESH,
            )
            copy.start()
            copies.append(copy)
        kept = pltpu.make_async_copy(value if gather else value.at[mine], result.at[mine], own)
        kept.start()
        kept.wait()
        for copy in copies:
            copy.wait()

    on_ring(body, axis)


def exchange(value, axis, number, gather=False):
    count = lax.axis_size(axis)
    shape = ((count,) + value.shape) if gather else value.shape
    return pl.pallas_call(
        functools.partial(exchange_kernel, axis, gather),
        out_shape=jax.ShapeDtypeStruct(shape, value.dtype),
        in_specs=[pl.BlockSpec(memory_space=pltpu.VMEM)],
        out_specs=pl.BlockSpec(memory_space=pltpu.VMEM),
        scratch_shapes=[
            pltpu.SemaphoreType.DMA((count,)),
            pltpu.SemaphoreType.DMA((count,)),
            pltpu.SemaphoreType.DMA,
        ],
        compiler_params=pltpu.CompilerParams(collective_id=number, has_side_effects=True),
        name=f"exchange_{number}",
    )(value)


def across(left, right):
    return lax.dot_general(
        left, right, (((1,), (1,)), ((), ())), preferred_element_type=jnp.float32
    )


def prepare(values, shift, maps, scale, drive_real, drive_imaginary):
    groups, width = shift.shape[1], scale.shape[1]
    spread = lax.broadcasted_iota(jnp.int32, (groups, width), 1) // (width // groups)
    hot = (spread == lax.broadcasted_iota(jnp.int32, (groups, width), 0)).astype(jnp.float32)
    scale[...] = jnp.dot(
        jnp.exp(shift[...]), hot, precision=TOP_PRECISION, preferred_element_type=jnp.float32
    )
    entries = values[...]
    drive_real[...] = across(entries, maps[0]) + across(entries, maps[1])
    drive_imaginary[...] = across(entries, maps[2]) + across(entries, maps[3])


def totals_kernel(values, shift, factor, maps, parts, total, scale, drive_real, drive_imaginary):
    prepare(values, shift, maps, scale, drive_real, drive_imaginary)
    width = scale.shape[1]
    wide = (LANES, width)
    factor_real = jnp.broadcast_to(factor[0:1, :], wide)
    factor_imaginary = jnp.broadcast_to(factor[1:2, :], wide)

    def step(position, carry):
        a_real, a_imaginary, x_real, x_imaginary = carry
        rows = pl.ds(pl.multiple_of(position * LANES, LANES), LANES)
        grow = scale[rows, :]
        b_real, b_imaginary = grow * factor_real, grow * factor_imaginary
        return (
            b_real * a_real - b_imaginary * a_imaginary,
            b_real * a_imaginary + b_imaginary * a_real,
            b_real * x_real - b_imaginary * x_imaginary + drive_real[rows, :],
            b_real * x_imaginary + b_imaginary * x_real + drive_imaginary[rows, :],
        )

    empty = jnp.zeros(wide, jnp.float32)
    ends = lax.fori_loop(
        0, scale.shape[0] // LANES, step, (jnp.ones(wide, jnp.float32), empty, empty, empty)
    )
    for place, end in enumerate(ends):
        parts[place] = end
    run = tuple(end[0:1] for end in ends)
    for segment in range(1, LANES):
        b_real, b_imaginary, y_real, y_imaginary = (
            end[segment : segment + 1] for end in ends
        )
        a_real, a_imaginary, x_real, x_imaginary = run
        run = (
            b_real * a_real - b_imaginary * a_imaginary,
            b_real * a_imaginary + b_imaginary * a_real,
            b_real * x_real - b_imaginary * x_imaginary + y_real,
            b_real * x_imaginary + b_imaginary * x_real + y_imaginary,
        )
    total[...] = jnp.concatenate(run + (jnp.zeros((LANES - 4, width), jnp.float32),), axis=0)


def split(value):
    high = value.astype(jnp.bfloat16)
    return high, (value - high.astype(jnp.float32)).astype(jnp.bfloat16)


def respond_kernel(
    axis, values, shift, factor, maps, parts, gathered, reads, skip, out,
    scale, drive_real, drive_imaginary,
):
    prepare(values, shift, maps, scale, drive_real, drive_imaginary)
    width = scale.shape[1]
    mine = lax.axis_index(axis)

    def before(position, carry):
        real, imaginary = carry
        item = gathered[position]
        a_real, a_imaginary = item[0:1], item[1:2]
        keep = position < mine
        return (
            jnp.where(keep, a_real * real - a_imaginary * imaginary + item[2:3], real),
            jnp.where(keep, a_real * imaginary + a_imaginary * real + item[3:4], imaginary),
        )

    none = jnp.zeros((1, width), jnp.float32)
    real, imaginary = lax.fori_loop(0, gathered.shape[0] - 1, before, (none, none))
    reals, imaginaries = [real], [imaginary]
    for segment in range(LANES - 1):
        at = slice(segment, segment + 1)
        a_real, a_imaginary = parts[0, at, :], parts[1, at, :]
        real, imaginary = (
            a_real * real - a_imaginary * imaginary + parts[2, at, :],
            a_real * imaginary + a_imaginary * real + parts[3, at, :],
        )
        reals.append(real)
        imaginaries.append(imaginary)
    wide = (LANES, width)
    factor_real = jnp.broadcast_to(factor[0:1, :], wide)
    factor_imaginary = jnp.broadcast_to(factor[1:2, :], wide)

    def step(position, carry):
        x_real, x_imaginary = carry
        rows = pl.ds(pl.multiple_of(position * LANES, LANES), LANES)
        grow = scale[rows, :]
        b_real, b_imaginary = grow * factor_real, grow * factor_imaginary
        new_real = b_real * x_real - b_imaginary * x_imaginary + drive_real[rows, :]
        new_imaginary = b_real * x_imaginary + b_imaginary * x_real + drive_imaginary[rows, :]
        drive_real[rows, :] = new_real
        drive_imaginary[rows, :] = new_imaginary
        return new_real, new_imaginary

    lax.fori_loop(
        0,
        scale.shape[0] // LANES,
        step,
        (jnp.concatenate(reals, axis=0), jnp.concatenate(imaginaries, axis=0)),
    )
    high, low = split(drive_real[...])
    response = across(high, reads[0]) + across(low, reads[0]) + across(high, reads[1])
    high, low = split(drive_imaginary[...])
    response -= across(high, reads[2]) + across(low, reads[2]) + across(high, reads[3])
    response += skip[...] * values[...].astype(jnp.float32)
    out[...] = jax.nn.gelu(response).astype(jnp.bfloat16)


def diagonal(blocks):
    groups, rows, columns = blocks.shape
    tiled = jnp.tile(blocks.reshape(groups * rows, columns), (1, groups))
    row = lax.broadcasted_iota(jnp.int32, tiled.shape, 0) // rows
    column = lax.broadcasted_iota(jnp.int32, tiled.shape, 1) // columns
    return split(jnp.where(row == column, tiled, 0.0))


def mixer(mixer_input, decay_shift, factors, readout_matrix, skip):
    factor_real, factor_imaginary, map_real, map_imaginary = factors
    rows, channels = mixer_input.shape
    groups, states = factor_real.shape
    width = groups * states

    def arrange(value):
        return jnp.swapaxes(value.reshape(LANES, rows // LANES, -1), 0, 1).reshape(rows, -1)

    values, shift = arrange(mixer_input), arrange(decay_shift)
    factor = jnp.stack([factor_real.reshape(width), factor_imaginary.reshape(width)])
    maps = jnp.stack(diagonal(map_real) + diagonal(map_imaginary))
    reads = jnp.stack(
        diagonal(readout_matrix[0]) + diagonal(readout_matrix[1])
    )
    vmem = pl.BlockSpec(memory_space=pltpu.VMEM)
    scratch = [pltpu.VMEM((rows, width), jnp.float32)] * 3
    parts, total = pl.pallas_call(
        totals_kernel,
        out_shape=(
            jax.ShapeDtypeStruct((4, LANES, width), jnp.float32),
            jax.ShapeDtypeStruct((LANES, width), jnp.float32),
        ),
        in_specs=[vmem] * 4,
        out_specs=(vmem, vmem),
        scratch_shapes=scratch,
        name="totals",
    )(values, shift, factor, maps)
    gathered = exchange(total, "sp", 0, gather=True)
    activated = pl.pallas_call(
        functools.partial(respond_kernel, "sp"),
        out_shape=jax.ShapeDtypeStruct((rows, channels), jnp.bfloat16),
        in_specs=[vmem] * 8,
        out_specs=vmem,
        scratch_shapes=scratch,
        name="respond",
    )(values, shift, factor, maps, parts, gathered, reads, skip.reshape(1, -1))
    return jnp.swapaxes(activated.reshape(rows // LANES, LANES, channels), 0, 1)


def slot_numbers(route_rows, experts, capacity):
    flat = route_rows.reshape(route_rows.shape[:-2] + (-1,))
    matches = (flat[..., None] == jnp.arange(experts, dtype=jnp.int32)).astype(jnp.int32)
    earlier = jnp.cumsum(matches, axis=-2) - matches
    return flat * capacity + jnp.sum(earlier * matches, axis=-1)


def dispatch_rows(slots, normed, width):
    hits = (slots[..., None] == jnp.arange(width, dtype=jnp.int32)).astype(jnp.bfloat16)
    tokens = normed.shape[-2]
    hits = hits.reshape(slots.shape[:-1] + (tokens, -1, width)).sum(axis=-2)
    return jnp.einsum(
        "...tw,...td->...wd", hits, normed, preferred_element_type=jnp.float32
    ).astype(jnp.bfloat16)


def flip(index, bits):
    bit = 1
    while bit <= bits:
        if bits & bit:
            index = index + bit - 2 * bit * (index // bit % 2)
        bit *= 2
    return index


def plan(experts):
    if experts == 8:
        order, sends = (0, 1, 4, 2, 5, 6, 7, 3), (1, 4, 2, 5, 6, 7, 3)
        near, far = (0, 0, 0, 1, 6, 12, 15, 17), (0, 0, 5, 7, 12, 17, 20, 23)
    else:
        order, sends = tuple(range(experts)), tuple(range(1, experts))
        near = tuple(max(0, 4 * place - 12) for place in range(experts))
        far = tuple(max(0, 4 * place - 6) for place in range(experts))
    events = {slot: [] for slot in range(4 * experts)}
    for place in range(experts):
        if place > 1:
            events[near[place]].append(("pass_on", order[place]))
        if place > 0:
            events[far[place]].append(("pass_far", order[place]))
    late = []
    for place in range(experts):
        for name, slot in (("cross", 4 * place + 5), ("give_back", 4 * place + 10)):
            if slot < 4 * experts:
                events[slot].append((name, order[place]))
            else:
                late.append((slot, name, order[place]))
    return order, sends, events, [item[1:] for item in sorted(late)]


def same(shape, row, column):
    rows = lax.broadcasted_iota(jnp.int32, shape, 0)
    columns = lax.broadcasted_iota(jnp.int32, shape, 1)
    return row(rows) == column(columns)


def chain(later, earlier):
    b_real, b_imaginary, y_real, y_imaginary = later
    a_real, a_imaginary, x_real, x_imaginary = earlier
    return (
        b_real * a_real - b_imaginary * a_imaginary,
        b_real * a_imaginary + b_imaginary * a_real,
        b_real * x_real - b_imaginary * x_imaginary + y_real,
        b_real * x_imaginary + b_imaginary * x_real + y_imaginary,
    )


KINDS = ("sp", "y", "core", "far", "core_back", "y_back", "sp_back")
PARTS = 2


def layer_kernel(
    values_in, shift_in, real_in, imaginary_in, log_in, map_in, readout_in, skip_in, proj_in,
    stream_in, gain_in, routes_in, logits_in, w_gate, w_up, w_down, out,
    values, shift, pole_real, pole_imaginary, log_step, input_map, readout, skip,
    stream, gain, routes, logits,
    scale, drive_real, drive_imaginary, parts, total, gathered, activated, acts, proj,
    gate, up, down, outgoing, rows, hidden, kept, given, from_core, to_y, from_y, back, returned,
    in_sem, own_sem, tot_send, tot_recv, act_send, act_recv, proj_send, proj_recv,
    load_sem, send_sem, recv_sem,
):
    positions, width = scale.shape
    groups, states = pole_real.shape
    channels = values.shape[1]
    inner = channels // groups
    tokens, model = out.shape
    experts, capacity = outgoing.shape[:2]
    hidden_width = gate.shape[1]
    tile, wide_tile = hidden_width // 2, model // 2
    depth = channels // (2 * PARTS)
    place, share = lax.axis_index("sp"), lax.axis_index("tp")
    names = [flip(place, bits) for bits in range(experts)]
    shares = [flip(share, kind) for kind in range(4)]
    partner, across_y = shares[1], shares[2]
    order, sends, events, late = plan(experts)
    float_dot = functools.partial(
        jnp.dot, precision=TOP_PRECISION, preferred_element_type=jnp.float32
    )

    barrier = pltpu.get_barrier_semaphore()
    for bits in range(1, experts):
        pl.semaphore_signal(barrier, inc=1, device_id={"sp": names[bits]}, device_id_type=MESH)
    for kind in range(1, 4):
        pl.semaphore_signal(barrier, inc=1, device_id={"tp": shares[kind]}, device_id_type=MESH)

    inputs = (
        (values_in, values), (shift_in, shift), (real_in, pole_real),
        (imaginary_in, pole_imaginary), (log_in, log_step), (map_in, input_map),
        (readout_in, readout), (skip_in, skip), (stream_in, stream), (gain_in, gain),
        (routes_in, routes), (logits_in, logits),
    )
    fetches = [
        pltpu.make_async_copy(source, target, in_sem.at[number])
        for number, (source, target) in enumerate(inputs)
    ]
    for fetch in fetches:
        fetch.start()
    own_proj = pltpu.make_async_copy(proj_in, proj.at[0], own_sem)
    own_proj.start()

    def load(number, step):
        source, target = ((w_gate, gate), (w_up, up), (w_down, down))[number]
        length = wide_tile if number == 2 else tile
        columns = pl.ds(pl.multiple_of(step * length, 128), length)
        return pltpu.make_async_copy(
            source.at[:, columns], target.at[:, columns], load_sem.at[number, step]
        )

    def remote_copy(source, target, send, receive, peer):
        return pltpu.make_async_remote_copy(
            src_ref=source, dst_ref=target, send_sem=send, recv_sem=receive,
            device_id=peer, device_id_type=MESH,
        )

    half = place % 2

    def weights(kind, side, part):
        which = half if side == 0 else 1 - half
        start = pl.multiple_of((which * PARTS + part) * depth, depth)
        span = pl.ds(start, depth)
        number = part if kind == 4 else side * PARTS + part
        if kind == 4:
            source, target, peer = proj.at[2, span], proj.at[2, span], {"sp": names[1]}
        elif kind == 3:
            source, target, peer = proj.at[2, span], proj.at[3, span], {"tp": partner}
        else:
            source, target = proj_in.at[span], proj.at[kind, span]
            peer = {"tp": shares[kind]}
        return remote_copy(
            source, target, proj_send.at[kind, number], proj_recv.at[kind, number], peer
        )

    pl.semaphore_wait(barrier, experts + 2)
    for part in range(PARTS):
        weights(2, 0, part).start()
    for side in range(2):
        for part in range(PARTS):
            weights(1, side, part).start()
    for step in range(2):
        load(0, step).start()
        load(1, step).start()
    for step in range(2):
        load(2, step).start()
    for fetch in fetches:
        fetch.wait()

    spread = same((states, width), lambda r: r, lambda c: c % states)
    spread_low = spread.astype(jnp.bfloat16)
    group = same((groups, width), lambda r: r, lambda c: c // states)
    block = same((channels, width), lambda r: r // inner, lambda c: c // states)
    column = jnp.sum(
        jnp.where(same((groups, groups), lambda r: r, lambda c: c), log_step[...], 0.0),
        axis=1, keepdims=True,
    )
    real, imaginary = pole_real[...], pole_imaginary[...]
    step_size = jnp.exp(column)
    magnitude = jnp.exp(real * step_size)
    factor_real = magnitude * jnp.cos(imaginary * step_size)
    factor_imaginary = magnitude * jnp.sin(imaginary * step_size)
    denominator = real * real + imaginary * imaginary
    ratio_real = ((factor_real - 1.0) * real + factor_imaginary * imaginary) / denominator
    ratio_imaginary = (factor_imaginary * real - (factor_real - 1.0) * imaginary) / denominator
    ratio_real, ratio_imaginary = (
        jnp.broadcast_to(ratio[:, None, :], (groups, inner, states)).reshape(channels, states)
        for ratio in (ratio_real, ratio_imaginary)
    )
    map_real = ratio_real * input_map[0] - ratio_imaginary * input_map[1]
    map_imaginary = ratio_real * input_map[1] + ratio_imaginary * input_map[0]
    laid = float_dot(
        jnp.concatenate([factor_real, factor_imaginary], axis=0), spread.astype(jnp.float32)
    )
    factor_real, factor_imaginary = (
        jnp.sum(
            jnp.where(group, laid[n * groups : (n + 1) * groups], 0.0), axis=0, keepdims=True
        )
        for n in range(2)
    )

    segment = positions // LANES
    permute = same((positions, positions), lambda r: r % LANES * segment + r // LANES, lambda c: c)
    entries = jnp.dot(
        permute.astype(jnp.bfloat16), values[...], preferred_element_type=jnp.float32
    ).astype(jnp.bfloat16)
    growth = lax.dot_general(
        permute.astype(jnp.float32), jnp.exp(shift[...]), (((1,), (1,)), ((), ())),
        precision=TOP_PRECISION, preferred_element_type=jnp.float32,
    )
    scale[...] = float_dot(growth, group.astype(jnp.float32))

    def diagonal(value):
        return [
            jnp.where(
                block, jnp.dot(piece, spread_low, preferred_element_type=jnp.float32), 0.0
            ).astype(jnp.bfloat16)
            for piece in split(value)
        ]

    for target, value in ((drive_real, map_real), (drive_imaginary, map_imaginary)):
        high, low = diagonal(value)
        target[...] = jnp.dot(entries, high, preferred_element_type=jnp.float32) + jnp.dot(
            entries, low, preferred_element_type=jnp.float32
        )

    wide = (LANES, width)
    wide_real = jnp.broadcast_to(factor_real, wide)
    wide_imaginary = jnp.broadcast_to(factor_imaginary, wide)

    def first_pass(position, carry):
        at = pl.ds(pl.multiple_of(position * LANES, LANES), LANES)
        grow = scale[at, :]
        item = (
            grow * wide_real, grow * wide_imaginary, drive_real[at, :], drive_imaginary[at, :]
        )
        return chain(item, carry)

    empty = jnp.zeros(wide, jnp.float32)
    ends = lax.fori_loop(
        0, segment, first_pass, (jnp.ones(wide, jnp.float32), empty, empty, empty)
    )
    for number, end in enumerate(ends):
        parts[number] = end
    run = tuple(end[0:1] for end in ends)
    for number in range(1, LANES):
        run = chain(tuple(end[number : number + 1] for end in ends), run)
    total[...] = jnp.concatenate(run + (jnp.zeros((LANES - 4, width), jnp.float32),), axis=0)
    gathered[place] = total[...]

    def totals(bits):
        return remote_copy(
            total, gathered.at[place], tot_send.at[bits], tot_recv.at[bits], {"sp": names[bits]}
        )

    for bits in range(1, experts):
        totals(bits).start()
    reads = diagonal(readout[0]) + diagonal(readout[1])

    def share_out(part):
        weights(2, 0, part).wait_recv()
        weights(4, 0, part).start()
        weights(3, 0, part).start()

    share_out(0)
    for bits in range(1, experts):
        totals(bits).wait_recv()

    def before(position, carry):
        real, imaginary = carry
        item = gathered[position]
        a_real, a_imaginary = item[0:1], item[1:2]
        keep = position < place
        return (
            jnp.where(keep, a_real * real - a_imaginary * imaginary + item[2:3], real),
            jnp.where(keep, a_real * imaginary + a_imaginary * real + item[3:4], imaginary),
        )

    none = jnp.zeros((1, width), jnp.float32)
    real, imaginary = lax.fori_loop(0, experts - 1, before, (none, none))
    reals, imaginaries = [real], [imaginary]
    for number in range(LANES - 1):
        at = slice(number, number + 1)
        a_real, a_imaginary = parts[0, at, :], parts[1, at, :]
        real, imaginary = (
            a_real * real - a_imaginary * imaginary + parts[2, at, :],
            a_real * imaginary + a_imaginary * real + parts[3, at, :],
        )
        reals.append(real)
        imaginaries.append(imaginary)

    def second_pass(position, carry):
        x_real, x_imaginary = carry
        at = pl.ds(pl.multiple_of(position * LANES, LANES), LANES)
        grow = scale[at, :]
        b_real, b_imaginary = grow * wide_real, grow * wide_imaginary
        new_real = b_real * x_real - b_imaginary * x_imaginary + drive_real[at, :]
        new_imaginary = b_real * x_imaginary + b_imaginary * x_real + drive_imaginary[at, :]
        drive_real[at, :] = new_real
        drive_imaginary[at, :] = new_imaginary
        return new_real, new_imaginary

    lax.fori_loop(
        0,
        segment,
        second_pass,
        (jnp.concatenate(reals, axis=0), jnp.concatenate(imaginaries, axis=0)),
    )
    share_out(1)
    high, low = split(drive_real[...])
    response = across(high, reads[0]) + across(low, reads[0]) + across(high, reads[1])
    high, low = split(drive_imaginary[...])
    response -= across(high, reads[2]) + across(low, reads[2]) + across(high, reads[3])
    response += skip[...] * entries.astype(jnp.float32)
    restore = same((positions, positions), lambda r: r, lambda c: c % LANES * segment + c // LANES)
    activated[...] = jnp.dot(
        restore.astype(jnp.bfloat16),
        jax.nn.gelu(response).astype(jnp.bfloat16),
        preferred_element_type=jnp.float32,
    ).astype(jnp.bfloat16)

    def hand(kind):
        start = pl.multiple_of(shares[kind] * tokens, tokens)
        return remote_copy(
            activated.at[pl.ds(start, tokens)], acts.at[kind], act_send.at[kind],
            act_recv.at[kind], {"tp": shares[kind]},
        )

    for kind in range(1, 4):
        hand(kind).start()
    acts[0] = activated[pl.ds(pl.multiple_of(share * tokens, tokens), tokens), :]
    own_proj.wait()
    for part in range(PARTS):
        weights(4, 1, part).wait_recv()
        weights(3, 1, part).start()
    projected = jnp.dot(acts[0], proj[0], preferred_element_type=jnp.float32)
    for kind in range(1, 4):
        hand(kind).wait_recv()
        for side in range(2):
            for part in range(PARTS):
                if kind != 2:
                    weights(kind, side, part).wait_recv()
        projected += jnp.dot(acts[kind], proj[kind], preferred_element_type=jnp.float32)
    mixed = (stream[...].astype(jnp.float32) + projected).astype(jnp.bfloat16).astype(jnp.float32)
    normed = (
        mixed * lax.rsqrt(jnp.mean(mixed * mixed, axis=-1, keepdims=True) + EPS) * gain[...]
    ).astype(jnp.bfloat16)
    out[...] = mixed

    first, second = routes[0:1, :], routes[1:2, :]
    gap = logits[0:1, :] - logits[1:2, :]
    first_weight, second_weight = jax.nn.sigmoid(gap), jax.nn.sigmoid(-gap)
    named = jnp.concatenate(
        [((first == name) | (second == name)).astype(jnp.float32) for name in names], axis=0
    )
    earlier = (
        lax.broadcasted_iota(jnp.int32, (tokens, tokens), 0)
        < lax.broadcasted_iota(jnp.int32, (tokens, tokens), 1)
    ).astype(jnp.float32)
    rank = jnp.dot(named, earlier, preferred_element_type=jnp.float32).astype(jnp.int32)
    scale = jnp.concatenate(
        [
            jnp.where(first == name, first_weight, 0.0)
            + jnp.where(second == name, second_weight, 0.0)
            for name in names
        ],
        axis=0,
    )
    slot = lax.broadcasted_iota(jnp.int32, (capacity, tokens), 0)
    hits = [
        jnp.where(slot == rank[e : e + 1, :], named[e : e + 1, :], 0.0) for e in range(experts)
    ]
    combine = jnp.concatenate([hit * scale[e : e + 1, :] for e, hit in enumerate(hits)], axis=0)
    outgoing[...] = (
        jnp.dot(
            jnp.concatenate(hits, axis=0).astype(jnp.bfloat16),
            normed,
            preferred_element_type=jnp.float32,
        )
        .astype(jnp.bfloat16)
        .reshape(outgoing.shape)
    )
    spot = (0, 2, 1, 3)

    def at(bits, kind):
        return rows.at[bits, pl.ds(spot[kind] * capacity, capacity)]

    def remote(kind, bits):
        source, target, peer = {
            "sp": lambda: (outgoing.at[bits], at(bits, 0), {"sp": names[bits]}),
            "y": lambda: (at(bits, 0), at(bits, 2), {"tp": across_y}),
            "core": lambda: (at(bits, 0), at(bits, 1), {"tp": partner}),
            "far": lambda: (at(bits, 2), at(bits, 3), {"tp": partner}),
            "core_back": lambda: (given.at[bits], from_core.at[bits], {"tp": partner}),
            "y_back": lambda: (to_y.at[bits], from_y.at[bits], {"tp": across_y}),
            "sp_back": lambda: (back.at[bits], returned.at[bits], {"sp": names[bits]}),
        }[kind]()
        if bits == 0 and kind in ("y", "core"):
            source = outgoing.at[0]
        number = KINDS.index(kind)
        return remote_copy(
            source, target, send_sem.at[number, bits], recv_sem.at[number, bits], peer
        )

    def pass_on(bits):
        if bits:
            remote("sp", bits).wait_recv()
        remote("y", bits).start()
        remote("core", bits).start()

    def pass_far(bits):
        remote("y", bits).wait_recv()
        remote("far", bits).start()

    def cross(bits):
        remote("core_back", bits).wait_recv()
        to_y[bits] = (
            kept[bits, capacity:, :] + from_core[bits, capacity:, :].astype(jnp.float32)
        ).astype(jnp.bfloat16)
        remote("y_back", bits).start()

    def give_back(bits):
        remote("y_back", bits).wait_recv()
        total = (
            kept[bits, :capacity, :]
            + from_core[bits, :capacity, :].astype(jnp.float32)
            + from_y[bits].astype(jnp.float32)
        ).astype(jnp.bfloat16)
        if bits:
            back[bits] = total
            remote("sp_back", bits).start()
        else:
            returned[0] = total

    deeds = {"pass_on": pass_on, "pass_far": pass_far, "cross": cross, "give_back": give_back}

    def act(step, slots):
        for number, slot in enumerate(slots):
            if events[slot]:
                @pl.when(step == number)
                def _():
                    for name, bits in events[slot]:
                        deeds[name](bits)

    pass_on(0)
    for bits in sends:
        remote("sp", bits).start()
    rows[0, 0:capacity, :] = outgoing[0]
    pass_on(order[1])
    pass_far(0)
    for number, bits in enumerate(order):
        remote("core", bits).wait_recv()
        remote("far", bits).wait_recv()

        def widen(step, carry):
            columns = pl.ds(pl.multiple_of(step * tile, 128), tile)
            if number == 0:
                load(0, step).wait()
                load(1, step).wait()
            value = rows[bits]
            opened = jnp.dot(value, gate[:, columns], preferred_element_type=jnp.float32)
            raised = jnp.dot(value, up[:, columns], preferred_element_type=jnp.float32)
            hidden[:, columns] = (jax.nn.silu(opened) * raised).astype(jnp.bfloat16)
            act(step, (4 * number, 4 * number + 1))
            return carry

        lax.fori_loop(0, 2, widen, 0)

        def narrow(step, carry):
            columns = pl.ds(pl.multiple_of(step * wide_tile, 128), wide_tile)
            if number == 0:
                load(2, step).wait()
            value = jnp.dot(hidden[...], down[:, columns], preferred_element_type=jnp.float32)
            kept[bits, :, columns] = value[: 2 * capacity]
            given[bits, :, columns] = value[2 * capacity :].astype(jnp.bfloat16)
            act(step, (4 * number + 2, 4 * number + 3))
            return carry

        lax.fori_loop(0, 2, narrow, 0)
        remote("core_back", bits).start()
    for name, bits in late:
        deeds[name](bits)
    for bits in sends:
        remote("sp_back", bits).wait_recv()
    result = out[...]
    every = returned[...].reshape(experts * capacity, model)
    for piece in split(combine):
        result += lax.dot_general(
            piece, every, (((0,), (0,)), ((), ())), preferred_element_type=jnp.float32
        )
    out[...] = result
    for bits in range(experts):
        for kind in KINDS:
            if bits or kind not in ("sp", "sp_back"):
                remote(kind, bits).wait_send()
    for bits in range(1, experts):
        totals(bits).wait_send()
    for kind in range(1, 4):
        hand(kind).wait_send()
    for side in range(2):
        for part in range(PARTS):
            weights(1, side, part).wait_send()
            weights(3, side, part).wait_send()
    for part in range(PARTS):
        weights(2, 0, part).wait_send()
        weights(4, 0, part).wait_send()


def fits(shares, experts, capacity, w_gate):
    if shares != 4 or w_gate.shape[0] != 1 or experts & (experts - 1) or experts < 2:
        return False
    return capacity % 16 == 0 and w_gate.shape[2] % 256 == 0 and w_gate.shape[1] % 256 == 0


def layer(operands, number):
    (values, shift, pole_real, pole_imaginary, log_step, input_map, readout, skip, out_proj,
     stream, gain, routes, logits, w_gate, w_up, w_down) = operands
    positions, channels = values.shape
    groups, states = pole_real.shape
    width = groups * states
    experts = lax.axis_size("sp")
    tokens, model = stream.shape
    capacity = 4 * tokens // experts
    hidden_width = w_gate.shape[1]
    bf16, f32 = jnp.bfloat16, jnp.float32
    dma = pltpu.SemaphoreType.DMA
    inputs = (
        values, shift, pole_real, pole_imaginary, log_step, input_map, readout, skip, stream,
        gain, routes, logits,
    )
    arrays = [
        ((positions, width), f32), ((positions, width), f32), ((positions, width), f32),
        ((4, LANES, width), f32), ((LANES, width), f32), ((experts, LANES, width), f32),
        ((positions, channels), bf16), ((4, tokens, channels), bf16), ((4, channels, model), bf16),
        ((model, hidden_width), bf16), ((model, hidden_width), bf16), ((hidden_width, model), bf16),
        ((experts, capacity, model), bf16), ((experts, 4 * capacity, model), bf16),
        ((4 * capacity, hidden_width), bf16), ((experts, 2 * capacity, model), f32),
        ((experts, 2 * capacity, model), bf16), ((experts, 2 * capacity, model), bf16),
    ] + [((experts, capacity, model), bf16)] * 4
    return pl.pallas_call(
        layer_kernel,
        out_shape=jax.ShapeDtypeStruct((tokens, model), f32),
        in_specs=[pl.BlockSpec(memory_space=pl.ANY)] * len(operands),
        out_specs=pl.BlockSpec(memory_space=pltpu.VMEM),
        scratch_shapes=[pltpu.VMEM(value.shape, value.dtype) for value in inputs]
        + [pltpu.VMEM(shape, kind) for shape, kind in arrays]
        + [
            dma((len(inputs),)), dma, dma((experts,)), dma((experts,)), dma((4,)), dma((4,)),
            dma((5, 2 * PARTS)), dma((5, 2 * PARTS)), dma((3, 2)),
            dma((len(KINDS), experts)), dma((len(KINDS), experts)),
        ],
        compiler_params=pltpu.CompilerParams(
            collective_id=number, has_side_effects=True, vmem_limit_bytes=63 * 2**20
        ),
        name="layer",
    )(*operands)


def shards(
    mixer_input,
    decay_shift,
    pole_real,
    pole_imaginary,
    log_step,
    input_map,
    readout_matrix,
    skip,
    out_proj,
    stream,
    norm_gain,
    routes,
    route_logits,
    w_gate,
    w_up,
    w_down,
):
    shares = lax.axis_size("tp")
    own_rows = stream.shape[0]
    experts = lax.axis_size("sp") * w_gate.shape[0]
    capacity = 4 * own_rows // experts
    if fits(shares, experts, capacity, w_gate):
        channels, (groups, states) = mixer_input.shape[1], pole_real.shape
        operands = (
            mixer_input, decay_shift.T, pole_real, pole_imaginary, log_step.reshape(1, -1),
            jnp.swapaxes(input_map, 2, 3).reshape(2, channels, states),
            readout_matrix.reshape(2, channels, states), skip.reshape(1, -1), out_proj, stream,
            norm_gain.reshape(1, -1), routes.T, route_logits.T, w_gate[0], w_up[0], w_down[0],
        )
        return layer(operands, 4).astype(jnp.bfloat16)
    factors = discretize(pole_real, pole_imaginary, log_step, input_map)
    activated = mixer(mixer_input, decay_shift, factors, readout_matrix, skip)
    whole_proj = lax.all_gather(out_proj, "tp", axis=0, tiled=True)
    received = exchange(activated.reshape(shares, own_rows, -1), "tp", 1)
    own_activated = jnp.swapaxes(received, 0, 1).reshape(own_rows, -1)
    projected = jnp.dot(own_activated, whole_proj, preferred_element_type=jnp.float32)
    mixed = (stream.astype(jnp.float32) + projected).astype(jnp.bfloat16)
    mixed_wide = mixed.astype(jnp.float32)
    normed = (
        mixed_wide
        * lax.rsqrt(jnp.mean(mixed_wide * mixed_wide, axis=-1, keepdims=True) + EPS)
        * norm_gain
    ).astype(jnp.bfloat16)
    weights = jax.nn.sigmoid(
        jnp.stack(
            [route_logits[:, 0] - route_logits[:, 1], route_logits[:, 1] - route_logits[:, 0]],
            axis=1,
        )
    )
    slot_width = experts * capacity
    model = stream.shape[1]
    own_slots = slot_numbers(routes, experts, capacity)
    outgoing = dispatch_rows(own_slots, normed, slot_width)
    arrived = exchange(outgoing.reshape(experts, capacity, model), "sp", 2)
    expert_rows = lax.all_gather(arrived.reshape(-1, model), "tp", axis=0, tiled=True)
    gate = jnp.dot(expert_rows, w_gate[0], preferred_element_type=jnp.float32)
    upward = jnp.dot(expert_rows, w_up[0], preferred_element_type=jnp.float32)
    hidden = (jax.nn.silu(gate) * upward).astype(jnp.bfloat16)
    summed = lax.psum_scatter(
        jnp.dot(hidden, w_down[0], preferred_element_type=jnp.float32).astype(jnp.bfloat16),
        "tp",
        scatter_dimension=0,
        tiled=True,
    )
    expert_out = summed.reshape(-1, capacity, model)
    returned_result = exchange(expert_out, "sp", 3).reshape(slot_width, model)
    picked = (
        jnp.take(returned_result, own_slots, axis=0)
        .astype(jnp.float32)
        .reshape(own_rows, -1, model)
    )
    combined = mixed_wide + jnp.sum(picked * weights[:, :, None], axis=1)
    return combined.astype(jnp.bfloat16)


def solution(mesh):
    return jax.shard_map(
        shards,
        mesh=mesh,
        in_specs=(
            P("sp", "tp"),
            P("sp", "tp"),
            P("tp", None),
            P("tp", None),
            P("tp"),
            P(None, "tp", None, None),
            P(None, "tp", None, None),
            P("tp"),
            P("tp", None),
            P(("sp", "tp"), None),
            P(),
            P(("sp", "tp"), None),
            P(("sp", "tp"), None),
            P("sp", None, "tp"),
            P("sp", None, "tp"),
            P("sp", "tp", None),
        ),
        out_specs=P(("sp", "tp"), None),
        check_vma=False,
    )
```

```python
import functools

import jax
import jax.numpy as jnp
from jax import lax
from jax.experimental import pallas as pl
from jax.experimental.pallas import tpu as pltpu
from jax.sharding import PartitionSpec as P

TOP_PRECISION = lax.Precision.HIGHEST
EPS = 1e-06
LANES = 8
MESH = pl.DeviceIdType.MESH


def discretize(pole_real, pole_imaginary, log_step, input_map):
    step = jnp.exp(log_step)[:, None]
    magnitude = jnp.exp(pole_real * step)
    factor_real = magnitude * jnp.cos(pole_imaginary * step)
    factor_imaginary = magnitude * jnp.sin(pole_imaginary * step)
    denominator = pole_real * pole_real + pole_imaginary * pole_imaginary
    ratio_real = ((factor_real - 1.0) * pole_real + factor_imaginary * pole_imaginary) / denominator
    ratio_imaginary = (
        factor_imaginary * pole_real - (factor_real - 1.0) * pole_imaginary
    ) / denominator
    map_real = ratio_real[:, :, None] * input_map[0] - ratio_imaginary[:, :, None] * input_map[1]
    map_imaginary = (
        ratio_real[:, :, None] * input_map[1] + ratio_imaginary[:, :, None] * input_map[0]
    )
    return (factor_real, factor_imaginary, map_real, map_imaginary)


def on_ring(body, axis):
    count, mine = lax.axis_size(axis), lax.axis_index(axis)
    barrier = pltpu.get_barrier_semaphore()
    for ahead in range(1, count):
        pl.semaphore_signal(
            barrier,
            inc=1,
            device_id={axis: lax.rem(mine + ahead, count)},
            device_id_type=MESH,
        )
    pl.semaphore_wait(barrier, count - 1)
    body(count, mine)


def exchange_kernel(axis, gather, value, result, send, receive, own):
    def body(count, mine):
        copies = []
        for ahead in range(1, count):
            peer = lax.rem(mine + ahead, count)
            copy = pltpu.make_async_remote_copy(
                src_ref=value if gather else value.at[peer],
                dst_ref=result.at[mine],
                send_sem=send.at[ahead],
                recv_sem=receive.at[ahead],
                device_id={axis: peer},
                device_id_type=MESH,
            )
            copy.start()
            copies.append(copy)
        kept = pltpu.make_async_copy(value if gather else value.at[mine], result.at[mine], own)
        kept.start()
        kept.wait()
        for copy in copies:
            copy.wait()

    on_ring(body, axis)


def exchange(value, axis, number, gather=False):
    count = lax.axis_size(axis)
    shape = ((count,) + value.shape) if gather else value.shape
    return pl.pallas_call(
        functools.partial(exchange_kernel, axis, gather),
        out_shape=jax.ShapeDtypeStruct(shape, value.dtype),
        in_specs=[pl.BlockSpec(memory_space=pltpu.VMEM)],
        out_specs=pl.BlockSpec(memory_space=pltpu.VMEM),
        scratch_shapes=[
            pltpu.SemaphoreType.DMA((count,)),
            pltpu.SemaphoreType.DMA((count,)),
            pltpu.SemaphoreType.DMA,
        ],
        compiler_params=pltpu.CompilerParams(collective_id=number, has_side_effects=True),
        name=f"exchange_{number}",
    )(value)


def across(left, right):
    return lax.dot_general(
        left, right, (((1,), (1,)), ((), ())), preferred_element_type=jnp.float32
    )


def prepare(values, shift, maps, scale, drive_real, drive_imaginary):
    groups, width = shift.shape[1], scale.shape[1]
    spread = lax.broadcasted_iota(jnp.int32, (groups, width), 1) // (width // groups)
    hot = (spread == lax.broadcasted_iota(jnp.int32, (groups, width), 0)).astype(jnp.float32)
    scale[...] = jnp.dot(
        jnp.exp(shift[...]), hot, precision=TOP_PRECISION, preferred_element_type=jnp.float32
    )
    entries = values[...]
    drive_real[...] = across(entries, maps[0]) + across(entries, maps[1])
    drive_imaginary[...] = across(entries, maps[2]) + across(entries, maps[3])


def totals_kernel(values, shift, factor, maps, parts, total, scale, drive_real, drive_imaginary):
    prepare(values, shift, maps, scale, drive_real, drive_imaginary)
    width = scale.shape[1]
    wide = (LANES, width)
    factor_real = jnp.broadcast_to(factor[0:1, :], wide)
    factor_imaginary = jnp.broadcast_to(factor[1:2, :], wide)

    def step(position, carry):
        a_real, a_imaginary, x_real, x_imaginary = carry
        rows = pl.ds(pl.multiple_of(position * LANES, LANES), LANES)
        grow = scale[rows, :]
        b_real, b_imaginary = grow * factor_real, grow * factor_imaginary
        return (
            b_real * a_real - b_imaginary * a_imaginary,
            b_real * a_imaginary + b_imaginary * a_real,
            b_real * x_real - b_imaginary * x_imaginary + drive_real[rows, :],
            b_real * x_imaginary + b_imaginary * x_real + drive_imaginary[rows, :],
        )

    empty = jnp.zeros(wide, jnp.float32)
    ends = lax.fori_loop(
        0, scale.shape[0] // LANES, step, (jnp.ones(wide, jnp.float32), empty, empty, empty)
    )
    for place, end in enumerate(ends):
        parts[place] = end
    run = tuple(end[0:1] for end in ends)
    for segment in range(1, LANES):
        b_real, b_imaginary, y_real, y_imaginary = (
            end[segment : segment + 1] for end in ends
        )
        a_real, a_imaginary, x_real, x_imaginary = run
        run = (
            b_real * a_real - b_imaginary * a_imaginary,
            b_real * a_imaginary + b_imaginary * a_real,
            b_real * x_real - b_imaginary * x_imaginary + y_real,
            b_real * x_imaginary + b_imaginary * x_real + y_imaginary,
        )
    total[...] = jnp.concatenate(run + (jnp.zeros((LANES - 4, width), jnp.float32),), axis=0)


def split(value):
    high = value.astype(jnp.bfloat16)
    return high, (value - high.astype(jnp.float32)).astype(jnp.bfloat16)


def respond_kernel(
    axis, values, shift, factor, maps, parts, gathered, reads, skip, out,
    scale, drive_real, drive_imaginary,
):
    prepare(values, shift, maps, scale, drive_real, drive_imaginary)
    width = scale.shape[1]
    mine = lax.axis_index(axis)

    def before(position, carry):
        real, imaginary = carry
        item = gathered[position]
        a_real, a_imaginary = item[0:1], item[1:2]
        keep = position < mine
        return (
            jnp.where(keep, a_real * real - a_imaginary * imaginary + item[2:3], real),
            jnp.where(keep, a_real * imaginary + a_imaginary * real + item[3:4], imaginary),
        )

    none = jnp.zeros((1, width), jnp.float32)
    real, imaginary = lax.fori_loop(0, gathered.shape[0] - 1, before, (none, none))
    reals, imaginaries = [real], [imaginary]
    for segment in range(LANES - 1):
        at = slice(segment, segment + 1)
        a_real, a_imaginary = parts[0, at, :], parts[1, at, :]
        real, imaginary = (
            a_real * real - a_imaginary * imaginary + parts[2, at, :],
            a_real * imaginary + a_imaginary * real + parts[3, at, :],
        )
        reals.append(real)
        imaginaries.append(imaginary)
    wide = (LANES, width)
    factor_real = jnp.broadcast_to(factor[0:1, :], wide)
    factor_imaginary = jnp.broadcast_to(factor[1:2, :], wide)

    def step(position, carry):
        x_real, x_imaginary = carry
        rows = pl.ds(pl.multiple_of(position * LANES, LANES), LANES)
        grow = scale[rows, :]
        b_real, b_imaginary = grow * factor_real, grow * factor_imaginary
        new_real = b_real * x_real - b_imaginary * x_imaginary + drive_real[rows, :]
        new_imaginary = b_real * x_imaginary + b_imaginary * x_real + drive_imaginary[rows, :]
        drive_real[rows, :] = new_real
        drive_imaginary[rows, :] = new_imaginary
        return new_real, new_imaginary

    lax.fori_loop(
        0,
        scale.shape[0] // LANES,
        step,
        (jnp.concatenate(reals, axis=0), jnp.concatenate(imaginaries, axis=0)),
    )
    high, low = split(drive_real[...])
    response = across(high, reads[0]) + across(low, reads[0]) + across(high, reads[1])
    high, low = split(drive_imaginary[...])
    response -= across(high, reads[2]) + across(low, reads[2]) + across(high, reads[3])
    response += skip[...] * values[...].astype(jnp.float32)
    out[...] = jax.nn.gelu(response).astype(jnp.bfloat16)


def diagonal(blocks):
    groups, rows, columns = blocks.shape
    tiled = jnp.tile(blocks.reshape(groups * rows, columns), (1, groups))
    row = lax.broadcasted_iota(jnp.int32, tiled.shape, 0) // rows
    column = lax.broadcasted_iota(jnp.int32, tiled.shape, 1) // columns
    return split(jnp.where(row == column, tiled, 0.0))


def mixer(mixer_input, decay_shift, factors, readout_matrix, skip):
    factor_real, factor_imaginary, map_real, map_imaginary = factors
    rows, channels = mixer_input.shape
    groups, states = factor_real.shape
    width = groups * states

    def arrange(value):
        return jnp.swapaxes(value.reshape(LANES, rows // LANES, -1), 0, 1).reshape(rows, -1)

    values, shift = arrange(mixer_input), arrange(decay_shift)
    factor = jnp.stack([factor_real.reshape(width), factor_imaginary.reshape(width)])
    maps = jnp.stack(diagonal(map_real) + diagonal(map_imaginary))
    reads = jnp.stack(
        diagonal(readout_matrix[0]) + diagonal(readout_matrix[1])
    )
    vmem = pl.BlockSpec(memory_space=pltpu.VMEM)
    scratch = [pltpu.VMEM((rows, width), jnp.float32)] * 3
    parts, total = pl.pallas_call(
        totals_kernel,
        out_shape=(
            jax.ShapeDtypeStruct((4, LANES, width), jnp.float32),
            jax.ShapeDtypeStruct((LANES, width), jnp.float32),
        ),
        in_specs=[vmem] * 4,
        out_specs=(vmem, vmem),
        scratch_shapes=scratch,
        name="totals",
    )(values, shift, factor, maps)
    gathered = exchange(total, "sp", 0, gather=True)
    activated = pl.pallas_call(
        functools.partial(respond_kernel, "sp"),
        out_shape=jax.ShapeDtypeStruct((rows, channels), jnp.bfloat16),
        in_specs=[vmem] * 8,
        out_specs=vmem,
        scratch_shapes=scratch,
        name="respond",
    )(values, shift, factor, maps, parts, gathered, reads, skip.reshape(1, -1))
    return jnp.swapaxes(activated.reshape(rows // LANES, LANES, channels), 0, 1)


def slot_numbers(route_rows, experts, capacity):
    flat = route_rows.reshape(route_rows.shape[:-2] + (-1,))
    matches = (flat[..., None] == jnp.arange(experts, dtype=jnp.int32)).astype(jnp.int32)
    earlier = jnp.cumsum(matches, axis=-2) - matches
    return flat * capacity + jnp.sum(earlier * matches, axis=-1)


def dispatch_rows(slots, normed, width):
    hits = (slots[..., None] == jnp.arange(width, dtype=jnp.int32)).astype(jnp.bfloat16)
    tokens = normed.shape[-2]
    hits = hits.reshape(slots.shape[:-1] + (tokens, -1, width)).sum(axis=-2)
    return jnp.einsum(
        "...tw,...td->...wd", hits, normed, preferred_element_type=jnp.float32
    ).astype(jnp.bfloat16)


def flip(index, bits):
    bit = 1
    while bit <= bits:
        if bits & bit:
            index = index + bit - 2 * bit * (index // bit % 2)
        bit *= 2
    return index


def plan(experts):
    if experts == 8:
        order, sends = (0, 1, 4, 2, 5, 3, 6, 7), (4, 1, 2, 5, 3, 6, 7)
        near, far = (0, 0, 0, 1, 6, 9, 13, 17), (0, 0, 5, 7, 12, 14, 19, 22)
    else:
        order, sends = tuple(range(experts)), tuple(range(1, experts))
        near = tuple(max(0, 4 * place - 12) for place in range(experts))
        far = tuple(max(0, 4 * place - 6) for place in range(experts))
    events = {slot: [] for slot in range(4 * experts)}
    for place in range(experts):
        if place > 1:
            events[near[place]].append(("pass_on", order[place]))
        if place > 0:
            events[far[place]].append(("pass_far", order[place]))
    late = []
    for place in range(experts):
        for name, slot in (("cross", 4 * place + 5), ("give_back", 4 * place + 12)):
            if slot < 4 * experts:
                events[slot].append((name, order[place]))
            else:
                late.append((slot, name, order[place]))
    return order, sends, events, [item[1:] for item in sorted(late)]


def same(shape, row, column):
    rows = lax.broadcasted_iota(jnp.int32, shape, 0)
    columns = lax.broadcasted_iota(jnp.int32, shape, 1)
    return row(rows) == column(columns)


def chain(later, earlier):
    b_real, b_imaginary, y_real, y_imaginary = later
    a_real, a_imaginary, x_real, x_imaginary = earlier
    return (
        b_real * a_real - b_imaginary * a_imaginary,
        b_real * a_imaginary + b_imaginary * a_real,
        b_real * x_real - b_imaginary * x_imaginary + y_real,
        b_real * x_imaginary + b_imaginary * x_real + y_imaginary,
    )


KINDS = ("sp", "y", "core", "far", "core_back", "y_back", "sp_back")
PARTS = 2
PIECES = ((0, 0), (0, 1), (1, 0), (1, 1), (2, 0))


def layer_kernel(
    values_in, shift_in, real_in, imaginary_in, log_in, map_in, readout_in, skip_in, proj_in,
    stream_in, gain_in, routes_in, logits_in, w_gate, w_up, w_down, out,
    values, shift, pole_real, pole_imaginary, log_step, input_map, readout, skip,
    stream, gain, routes, logits,
    scale, drive_real, drive_imaginary, parts, total, gathered, activated, acts, proj,
    gate, up, down, outgoing, rows, hidden, kept, given, from_core, to_y, from_y, back, returned,
    in_sem, own_sem, tot_send, tot_recv, act_send, act_recv, proj_send, proj_recv,
    load_sem, send_sem, recv_sem,
):
    positions, width = scale.shape
    groups, states = pole_real.shape
    channels = values.shape[1]
    inner = channels // groups
    tokens, model = out.shape
    experts, capacity = outgoing.shape[:2]
    hidden_width = gate.shape[1]
    tile, wide_tile = hidden_width // 2, model // 2
    place, share = lax.axis_index("sp"), lax.axis_index("tp")
    names = [flip(place, bits) for bits in range(experts)]
    shares = [flip(share, kind) for kind in range(4)]
    partner, across_y = shares[1], shares[2]
    order, sends, events, late = plan(experts)
    float_dot = functools.partial(
        jnp.dot, precision=TOP_PRECISION, preferred_element_type=jnp.float32
    )

    barrier = pltpu.get_barrier_semaphore()
    for bits in range(1, experts):
        pl.semaphore_signal(barrier, inc=1, device_id={"sp": names[bits]}, device_id_type=MESH)
    for kind in range(1, 4):
        pl.semaphore_signal(barrier, inc=1, device_id={"tp": shares[kind]}, device_id_type=MESH)

    inputs = (
        (values_in, values), (shift_in, shift), (real_in, pole_real),
        (imaginary_in, pole_imaginary), (log_in, log_step), (map_in, input_map),
        (readout_in, readout), (skip_in, skip), (stream_in, stream), (gain_in, gain),
        (routes_in, routes), (logits_in, logits),
    )
    fetches = [
        pltpu.make_async_copy(source, target, in_sem.at[number])
        for number, (source, target) in enumerate(inputs)
    ]
    for fetch in fetches:
        fetch.start()
    own_proj = pltpu.make_async_copy(proj_in, proj.at[0], own_sem)
    own_proj.start()

    def load(number, step):
        source, target = ((w_gate, gate), (w_up, up), (w_down, down))[number]
        length = wide_tile if number == 2 else tile
        columns = pl.ds(pl.multiple_of(step * length, 128), length)
        return pltpu.make_async_copy(
            source.at[:, columns], target.at[:, columns], load_sem.at[number, step]
        )

    def remote_copy(source, target, send, receive, peer):
        return pltpu.make_async_remote_copy(
            src_ref=source, dst_ref=target, send_sem=send, recv_sem=receive,
            device_id=peer, device_id_type=MESH,
        )

    half = place % 2
    unit = channels // 16

    def weights(kind, side, part):
        if kind == 1:
            span = pl.ds(0, channels)
        elif side == 2:
            span = pl.ds(6 * unit, 4 * unit)
        else:
            which = half if side == 0 else 1 - half
            start = pl.multiple_of(which * 10 * unit + part * 3 * unit, unit)
            span = pl.ds(start, 3 * unit)
        number = part if kind == 4 else side * PARTS + part
        if kind == 4:
            source, target, peer = proj.at[2, span], proj.at[2, span], {"sp": names[1]}
        elif kind == 3:
            source, target, peer = proj.at[2, span], proj.at[3, span], {"tp": partner}
        else:
            source, target = proj_in.at[span], proj.at[kind, span]
            peer = {"tp": shares[kind]}
        return remote_copy(
            source, target, proj_send.at[kind, number], proj_recv.at[kind, number], peer
        )

    pl.semaphore_wait(barrier, experts + 2)
    for side, part in ((0, 0), (0, 1), (2, 0)):
        weights(2, side, part).start()
    weights(1, 0, 0).start()
    for step in range(2):
        load(0, step).start()
        load(1, step).start()
    for step in range(2):
        load(2, step).start()
    for fetch in fetches:
        fetch.wait()

    spread = same((states, width), lambda r: r, lambda c: c % states)
    spread_low = spread.astype(jnp.bfloat16)
    group = same((groups, width), lambda r: r, lambda c: c // states)
    block = same((channels, width), lambda r: r // inner, lambda c: c // states)
    column = jnp.sum(
        jnp.where(same((groups, groups), lambda r: r, lambda c: c), log_step[...], 0.0),
        axis=1, keepdims=True,
    )
    real, imaginary = pole_real[...], pole_imaginary[...]
    step_size = jnp.exp(column)
    magnitude = jnp.exp(real * step_size)
    factor_real = magnitude * jnp.cos(imaginary * step_size)
    factor_imaginary = magnitude * jnp.sin(imaginary * step_size)
    denominator = real * real + imaginary * imaginary
    ratio_real = ((factor_real - 1.0) * real + factor_imaginary * imaginary) / denominator
    ratio_imaginary = (factor_imaginary * real - (factor_real - 1.0) * imaginary) / denominator
    ratio_real, ratio_imaginary = (
        jnp.broadcast_to(ratio[:, None, :], (groups, inner, states)).reshape(channels, states)
        for ratio in (ratio_real, ratio_imaginary)
    )
    map_real = ratio_real * input_map[0] - ratio_imaginary * input_map[1]
    map_imaginary = ratio_real * input_map[1] + ratio_imaginary * input_map[0]
    laid = float_dot(
        jnp.concatenate([factor_real, factor_imaginary], axis=0), spread.astype(jnp.float32)
    )
    factor_real, factor_imaginary = (
        jnp.sum(
            jnp.where(group, laid[n * groups : (n + 1) * groups], 0.0), axis=0, keepdims=True
        )
        for n in range(2)
    )

    segment = positions // LANES
    permute = same((positions, positions), lambda r: r % LANES * segment + r // LANES, lambda c: c)
    entries = jnp.dot(
        permute.astype(jnp.bfloat16), values[...], preferred_element_type=jnp.float32
    ).astype(jnp.bfloat16)
    growth = lax.dot_general(
        permute.astype(jnp.float32), jnp.exp(shift[...]), (((1,), (1,)), ((), ())),
        precision=TOP_PRECISION, preferred_element_type=jnp.float32,
    )
    scale[...] = float_dot(growth, group.astype(jnp.float32))

    def diagonal(value):
        return [
            jnp.where(
                block, jnp.dot(piece, spread_low, preferred_element_type=jnp.float32), 0.0
            ).astype(jnp.bfloat16)
            for piece in split(value)
        ]

    for target, value in ((drive_real, map_real), (drive_imaginary, map_imaginary)):
        high, low = diagonal(value)
        target[...] = jnp.dot(entries, high, preferred_element_type=jnp.float32) + jnp.dot(
            entries, low, preferred_element_type=jnp.float32
        )

    wide = (LANES, width)
    wide_real = jnp.broadcast_to(factor_real, wide)
    wide_imaginary = jnp.broadcast_to(factor_imaginary, wide)

    def first_pass(position, carry):
        at = pl.ds(pl.multiple_of(position * LANES, LANES), LANES)
        grow = scale[at, :]
        item = (
            grow * wide_real, grow * wide_imaginary, drive_real[at, :], drive_imaginary[at, :]
        )
        return chain(item, carry)

    empty = jnp.zeros(wide, jnp.float32)
    ends = lax.fori_loop(
        0, segment, first_pass, (jnp.ones(wide, jnp.float32), empty, empty, empty)
    )
    for number, end in enumerate(ends):
        parts[number] = end
    run = tuple(end[0:1] for end in ends)
    for number in range(1, LANES):
        run = chain(tuple(end[number : number + 1] for end in ends), run)
    total[...] = jnp.concatenate(run + (jnp.zeros((LANES - 4, width), jnp.float32),), axis=0)
    gathered[place] = total[...]

    def totals(bits):
        return remote_copy(
            total, gathered.at[place], tot_send.at[bits], tot_recv.at[bits], {"sp": names[bits]}
        )

    for bits in range(1, experts):
        totals(bits).start()
    reads = diagonal(readout[0]) + diagonal(readout[1])

    def share_out(part):
        weights(2, 0, part).wait_recv()
        weights(4, 0, part).start()
        weights(3, 0, part).start()

    share_out(0)
    for bits in range(1, experts):
        totals(bits).wait_recv()

    def before(position, carry):
        real, imaginary = carry
        item = gathered[position]
        a_real, a_imaginary = item[0:1], item[1:2]
        keep = position < place
        return (
            jnp.where(keep, a_real * real - a_imaginary * imaginary + item[2:3], real),
            jnp.where(keep, a_real * imaginary + a_imaginary * real + item[3:4], imaginary),
        )

    none = jnp.zeros((1, width), jnp.float32)
    real, imaginary = lax.fori_loop(0, experts - 1, before, (none, none))
    reals, imaginaries = [real], [imaginary]
    for number in range(LANES - 1):
        at = slice(number, number + 1)
        a_real, a_imaginary = parts[0, at, :], parts[1, at, :]
        real, imaginary = (
            a_real * real - a_imaginary * imaginary + parts[2, at, :],
            a_real * imaginary + a_imaginary * real + parts[3, at, :],
        )
        reals.append(real)
        imaginaries.append(imaginary)

    def second_pass(position, carry):
        x_real, x_imaginary = carry
        at = pl.ds(pl.multiple_of(position * LANES, LANES), LANES)
        grow = scale[at, :]
        b_real, b_imaginary = grow * wide_real, grow * wide_imaginary
        new_real = b_real * x_real - b_imaginary * x_imaginary + drive_real[at, :]
        new_imaginary = b_real * x_imaginary + b_imaginary * x_real + drive_imaginary[at, :]
        drive_real[at, :] = new_real
        drive_imaginary[at, :] = new_imaginary
        return new_real, new_imaginary

    lax.fori_loop(
        0,
        segment,
        second_pass,
        (jnp.concatenate(reals, axis=0), jnp.concatenate(imaginaries, axis=0)),
    )
    share_out(1)
    high, low = split(drive_real[...])
    response = across(high, reads[0]) + across(low, reads[0]) + across(high, reads[1])
    high, low = split(drive_imaginary[...])
    response -= across(high, reads[2]) + across(low, reads[2]) + across(high, reads[3])
    response += skip[...] * entries.astype(jnp.float32)
    restore = same((positions, positions), lambda r: r, lambda c: c % LANES * segment + c // LANES)
    activated[...] = jnp.dot(
        restore.astype(jnp.bfloat16),
        jax.nn.gelu(response).astype(jnp.bfloat16),
        preferred_element_type=jnp.float32,
    ).astype(jnp.bfloat16)

    def hand(kind):
        start = pl.multiple_of(shares[kind] * tokens, tokens)
        return remote_copy(
            activated.at[pl.ds(start, tokens)], acts.at[kind], act_send.at[kind],
            act_recv.at[kind], {"tp": shares[kind]},
        )

    for kind in range(1, 4):
        hand(kind).start()
    acts[0] = activated[pl.ds(pl.multiple_of(share * tokens, tokens), tokens), :]
    own_proj.wait()
    weights(2, 2, 0).wait_recv()
    weights(3, 2, 0).start()
    for part in range(PARTS):
        weights(4, 1, part).wait_recv()
        weights(3, 1, part).start()
    projected = jnp.dot(acts[0], proj[0], preferred_element_type=jnp.float32)
    for kind in range(1, 4):
        hand(kind).wait_recv()
        if kind == 1:
            weights(1, 0, 0).wait_recv()
        if kind == 3:
            for side, part in PIECES:
                weights(3, side, part).wait_recv()
        projected += jnp.dot(acts[kind], proj[kind], preferred_element_type=jnp.float32)
    mixed = (stream[...].astype(jnp.float32) + projected).astype(jnp.bfloat16).astype(jnp.float32)
    normed = (
        mixed * lax.rsqrt(jnp.mean(mixed * mixed, axis=-1, keepdims=True) + EPS) * gain[...]
    ).astype(jnp.bfloat16)
    out[...] = mixed

    first, second = routes[0:1, :], routes[1:2, :]
    gap = logits[0:1, :] - logits[1:2, :]
    first_weight, second_weight = jax.nn.sigmoid(gap), jax.nn.sigmoid(-gap)
    named = jnp.concatenate(
        [((first == name) | (second == name)).astype(jnp.float32) for name in names], axis=0
    )
    earlier = (
        lax.broadcasted_iota(jnp.int32, (tokens, tokens), 0)
        < lax.broadcasted_iota(jnp.int32, (tokens, tokens), 1)
    ).astype(jnp.float32)
    rank = jnp.dot(named, earlier, preferred_element_type=jnp.float32).astype(jnp.int32)
    scale = jnp.concatenate(
        [
            jnp.where(first == name, first_weight, 0.0)
            + jnp.where(second == name, second_weight, 0.0)
            for name in names
        ],
        axis=0,
    )
    slot = lax.broadcasted_iota(jnp.int32, (capacity, tokens), 0)
    hits = [
        jnp.where(slot == rank[e : e + 1, :], named[e : e + 1, :], 0.0) for e in range(experts)
    ]
    combine = jnp.concatenate([hit * scale[e : e + 1, :] for e, hit in enumerate(hits)], axis=0)
    outgoing[...] = (
        jnp.dot(
            jnp.concatenate(hits, axis=0).astype(jnp.bfloat16),
            normed,
            preferred_element_type=jnp.float32,
        )
        .astype(jnp.bfloat16)
        .reshape(outgoing.shape)
    )
    spot = (0, 2, 1, 3)

    def at(bits, kind):
        return rows.at[bits, pl.ds(spot[kind] * capacity, capacity)]

    def remote(kind, bits):
        source, target, peer = {
            "sp": lambda: (outgoing.at[bits], at(bits, 0), {"sp": names[bits]}),
            "y": lambda: (at(bits, 0), at(bits, 2), {"tp": across_y}),
            "core": lambda: (at(bits, 0), at(bits, 1), {"tp": partner}),
            "far": lambda: (at(bits, 2), at(bits, 3), {"tp": partner}),
            "core_back": lambda: (given.at[bits], from_core.at[bits], {"tp": partner}),
            "y_back": lambda: (to_y.at[bits], from_y.at[bits], {"tp": across_y}),
            "sp_back": lambda: (back.at[bits], returned.at[bits], {"sp": names[bits]}),
        }[kind]()
        if bits == 0 and kind in ("y", "core"):
            source = outgoing.at[0]
        number = KINDS.index(kind)
        return remote_copy(
            source, target, send_sem.at[number, bits], recv_sem.at[number, bits], peer
        )

    def pass_on(bits):
        if bits:
            remote("sp", bits).wait_recv()
        remote("y", bits).start()
        remote("core", bits).start()

    def pass_far(bits):
        remote("y", bits).wait_recv()
        remote("far", bits).start()

    def cross(bits):
        remote("core_back", bits).wait_recv()
        to_y[bits] = (
            kept[bits, capacity:, :] + from_core[bits, capacity:, :].astype(jnp.float32)
        ).astype(jnp.bfloat16)
        remote("y_back", bits).start()

    def give_back(bits):
        remote("y_back", bits).wait_recv()
        total = (
            kept[bits, :capacity, :]
            + from_core[bits, :capacity, :].astype(jnp.float32)
            + from_y[bits].astype(jnp.float32)
        ).astype(jnp.bfloat16)
        if bits:
            back[bits] = total
            remote("sp_back", bits).start()
        else:
            returned[0] = total

    deeds = {"pass_on": pass_on, "pass_far": pass_far, "cross": cross, "give_back": give_back}

    def act(step, slots):
        for number, slot in enumerate(slots):
            if events[slot]:
                @pl.when(step == number)
                def _():
                    for name, bits in events[slot]:
                        deeds[name](bits)

    pass_on(0)
    for bits in sends:
        remote("sp", bits).start()
    rows[0, 0:capacity, :] = outgoing[0]
    pass_on(order[1])
    pass_far(0)
    for number, bits in enumerate(order):
        remote("core", bits).wait_recv()
        remote("far", bits).wait_recv()

        def widen(step, carry):
            columns = pl.ds(pl.multiple_of(step * tile, 128), tile)
            if number == 0:
                load(0, step).wait()
                load(1, step).wait()
            value = rows[bits]
            opened = jnp.dot(value, gate[:, columns], preferred_element_type=jnp.float32)
            raised = jnp.dot(value, up[:, columns], preferred_element_type=jnp.float32)
            hidden[:, columns] = (jax.nn.silu(opened) * raised).astype(jnp.bfloat16)
            act(step, (4 * number, 4 * number + 1))
            return carry

        lax.fori_loop(0, 2, widen, 0)

        def narrow(step, carry):
            columns = pl.ds(pl.multiple_of(step * wide_tile, 128), wide_tile)
            if number == 0:
                load(2, step).wait()
            value = jnp.dot(hidden[...], down[:, columns], preferred_element_type=jnp.float32)
            kept[bits, :, columns] = value[: 2 * capacity]
            given[bits, :, columns] = value[2 * capacity :].astype(jnp.bfloat16)
            act(step, (4 * number + 2, 4 * number + 3))
            return carry

        lax.fori_loop(0, 2, narrow, 0)
        remote("core_back", bits).start()
    for name, bits in late:
        deeds[name](bits)
    for bits in sends:
        remote("sp_back", bits).wait_recv()
    result = out[...]
    every = returned[...].reshape(experts * capacity, model)
    for piece in split(combine):
        result += lax.dot_general(
            piece, every, (((0,), (0,)), ((), ())), preferred_element_type=jnp.float32
        )
    out[...] = result
    for bits in range(experts):
        for kind in KINDS:
            if bits or kind not in ("sp", "sp_back"):
                remote(kind, bits).wait_send()
    for bits in range(1, experts):
        totals(bits).wait_send()
    for kind in range(1, 4):
        hand(kind).wait_send()
    weights(1, 0, 0).wait_send()
    for side, part in PIECES:
        weights(3, side, part).wait_send()
        if side != 1:
            weights(2, side, part).wait_send()
        if side == 0:
            weights(4, side, part).wait_send()


def fits(shares, experts, capacity, w_gate):
    if shares != 4 or w_gate.shape[0] != 1 or experts & (experts - 1) or experts < 2:
        return False
    return capacity % 16 == 0 and w_gate.shape[2] % 256 == 0 and w_gate.shape[1] % 256 == 0


def layer(operands, number):
    (values, shift, pole_real, pole_imaginary, log_step, input_map, readout, skip, out_proj,
     stream, gain, routes, logits, w_gate, w_up, w_down) = operands
    positions, channels = values.shape
    groups, states = pole_real.shape
    width = groups * states
    experts = lax.axis_size("sp")
    tokens, model = stream.shape
    capacity = 4 * tokens // experts
    hidden_width = w_gate.shape[1]
    bf16, f32 = jnp.bfloat16, jnp.float32
    dma = pltpu.SemaphoreType.DMA
    inputs = (
        values, shift, pole_real, pole_imaginary, log_step, input_map, readout, skip, stream,
        gain, routes, logits,
    )
    arrays = [
        ((positions, width), f32), ((positions, width), f32), ((positions, width), f32),
        ((4, LANES, width), f32), ((LANES, width), f32), ((experts, LANES, width), f32),
        ((positions, channels), bf16), ((4, tokens, channels), bf16), ((4, channels, model), bf16),
        ((model, hidden_width), bf16), ((model, hidden_width), bf16), ((hidden_width, model), bf16),
        ((experts, capacity, model), bf16), ((experts, 4 * capacity, model), bf16),
        ((4 * capacity, hidden_width), bf16), ((experts, 2 * capacity, model), f32),
        ((experts, 2 * capacity, model), bf16), ((experts, 2 * capacity, model), bf16),
    ] + [((experts, capacity, model), bf16)] * 4
    return pl.pallas_call(
        layer_kernel,
        out_shape=jax.ShapeDtypeStruct((tokens, model), f32),
        in_specs=[pl.BlockSpec(memory_space=pl.ANY)] * len(operands),
        out_specs=pl.BlockSpec(memory_space=pltpu.VMEM),
        scratch_shapes=[pltpu.VMEM(value.shape, value.dtype) for value in inputs]
        + [pltpu.VMEM(shape, kind) for shape, kind in arrays]
        + [
            dma((len(inputs),)), dma, dma((experts,)), dma((experts,)), dma((4,)), dma((4,)),
            dma((5, len(PIECES))), dma((5, len(PIECES))), dma((3, 2)),
            dma((len(KINDS), experts)), dma((len(KINDS), experts)),
        ],
        compiler_params=pltpu.CompilerParams(
            collective_id=number, has_side_effects=True, vmem_limit_bytes=63 * 2**20
        ),
        name="layer",
    )(*operands)


def shards(
    mixer_input,
    decay_shift,
    pole_real,
    pole_imaginary,
    log_step,
    input_map,
    readout_matrix,
    skip,
    out_proj,
    stream,
    norm_gain,
    routes,
    route_logits,
    w_gate,
    w_up,
    w_down,
):
    shares = lax.axis_size("tp")
    own_rows = stream.shape[0]
    experts = lax.axis_size("sp") * w_gate.shape[0]
    capacity = 4 * own_rows // experts
    if fits(shares, experts, capacity, w_gate):
        channels, (groups, states) = mixer_input.shape[1], pole_real.shape
        operands = (
            mixer_input, decay_shift.T, pole_real, pole_imaginary, log_step.reshape(1, -1),
            jnp.swapaxes(input_map, 2, 3).reshape(2, channels, states),
            readout_matrix.reshape(2, channels, states), skip.reshape(1, -1), out_proj, stream,
            norm_gain.reshape(1, -1), routes.T, route_logits.T, w_gate[0], w_up[0], w_down[0],
        )
        return layer(operands, 4).astype(jnp.bfloat16)
    factors = discretize(pole_real, pole_imaginary, log_step, input_map)
    activated = mixer(mixer_input, decay_shift, factors, readout_matrix, skip)
    whole_proj = lax.all_gather(out_proj, "tp", axis=0, tiled=True)
    received = exchange(activated.reshape(shares, own_rows, -1), "tp", 1)
    own_activated = jnp.swapaxes(received, 0, 1).reshape(own_rows, -1)
    projected = jnp.dot(own_activated, whole_proj, preferred_element_type=jnp.float32)
    mixed = (stream.astype(jnp.float32) + projected).astype(jnp.bfloat16)
    mixed_wide = mixed.astype(jnp.float32)
    normed = (
        mixed_wide
        * lax.rsqrt(jnp.mean(mixed_wide * mixed_wide, axis=-1, keepdims=True) + EPS)
        * norm_gain
    ).astype(jnp.bfloat16)
    weights = jax.nn.sigmoid(
        jnp.stack(
            [route_logits[:, 0] - route_logits[:, 1], route_logits[:, 1] - route_logits[:, 0]],
            axis=1,
        )
    )
    slot_width = experts * capacity
    model = stream.shape[1]
    own_slots = slot_numbers(routes, experts, capacity)
    outgoing = dispatch_rows(own_slots, normed, slot_width)
    arrived = exchange(outgoing.reshape(experts, capacity, model), "sp", 2)
    expert_rows = lax.all_gather(arrived.reshape(-1, model), "tp", axis=0, tiled=True)
    gate = jnp.dot(expert_rows, w_gate[0], preferred_element_type=jnp.float32)
    upward = jnp.dot(expert_rows, w_up[0], preferred_element_type=jnp.float32)
    hidden = (jax.nn.silu(gate) * upward).astype(jnp.bfloat16)
    summed = lax.psum_scatter(
        jnp.dot(hidden, w_down[0], preferred_element_type=jnp.float32).astype(jnp.bfloat16),
        "tp",
        scatter_dimension=0,
        tiled=True,
    )
    expert_out = summed.reshape(-1, capacity, model)
    returned_result = exchange(expert_out, "sp", 3).reshape(slot_width, model)
    picked = (
        jnp.take(returned_result, own_slots, axis=0)
        .astype(jnp.float32)
        .reshape(own_rows, -1, model)
    )
    combined = mixed_wide + jnp.sum(picked * weights[:, :, None], axis=1)
    return combined.astype(jnp.bfloat16)


def solution(mesh):
    return jax.shard_map(
        shards,
        mesh=mesh,
        in_specs=(
            P("sp", "tp"),
            P("sp", "tp"),
            P("tp", None),
            P("tp", None),
            P("tp"),
            P(None, "tp", None, None),
            P(None, "tp", None, None),
            P("tp"),
            P("tp", None),
            P(("sp", "tp"), None),
            P(),
            P(("sp", "tp"), None),
            P(("sp", "tp"), None),
            P("sp", None, "tp"),
            P("sp", None, "tp"),
            P("sp", "tp", None),
        ),
        out_specs=P(("sp", "tp"), None),
        check_vma=False,
    )
```
